256 devices in a mesh: gr: 2 (over z_hi), sp: 16 (over z_lo, y), tp: 8 (over x, core).
Axes of the slice: x: 4, y: 4, z: 8 (z_hi: 2, z_lo: 4; z = z_hi * 4 + z_lo), core: 2. Of those that a mesh axis runs over, the one named last changes fastest.
Arguments:
- context_input_tensor: bfloat16 [16, 16384, 2048], P(('gr', 'tp'), 'sp'), parts along dimension 0, may hold values from -8 to 8
- content_mapping_matrix: bfloat16 [2048, 1024], replicated, may hold values from -0.125 to 0.125
- address_mapping_matrix: bfloat16 [2048, 256], replicated, may hold values from -0.125 to 0.125
- increment_mapping_matrix: bfloat16 [2048, 16], replicated, may hold values from -0.125 to 0.125
- increment_speed_offset: float32 [16], P('sp'), may hold values from -1 to 0.5
- channel_fading_exponent: float32 [16], P('sp'), may hold values from -12 to -2
- extra_damping_spikes: float32 [16, 16, 16384], P(('gr', 'tp'), 'sp'), parts along dimension 0, may hold values from -3 to 0
- content_smoothing_coefficients: float32 [5, 16, 64], P(None, 'sp'), may hold values from -2.5 to 2.5
- address_smoothing_coefficients: float32 [5, 4, 64], replicated, may hold values from -2.5 to 2.5
- newest_lookup_matrix: bfloat16 [16, 4, 64], P(('gr', 'tp')), parts along dimension 0, may hold values from -6 to 6
- newest_output_switch: bfloat16 [16, 16, 64], P(('gr', 'tp'), 'sp'), parts along dimension 0, may hold values from -6 to 6
- cluster_scaling_coefficients: float32 [16, 64], P('sp'), may hold values from 0.1 to 1.9
Outputs:
- address_content_store: bfloat16 [16, 16384, 16, 128], P(('gr', 'tp'), None, 'sp'), parts along dimension 0
- earliest_switched_retrieval: bfloat16 [16, 16, 64], P(('gr', 'tp'), 'sp'), parts along dimension 0
The draws below stay inside these ranges and needn't reach their ends.
There are 2 independent parts, one for each index of `gr`. The reference program is written for one: setup_inputs(seed, part) draws one part's arguments, and reference() takes and returns one part's arrays. A program takes and returns all parts, laid end to end along the dimension named above; an argument that names none is the same for every part. Nothing has to cross between parts.
All inputs are finite; a program needn't handle non-finite values.
Results may differ from the reference program's by a relative error of at most 0.009.
Values may be sent and summed in bfloat16 or wider, within the bound.
A program may use at most 128 MiB of HBM per device.

```python
import math
import jax
import jax.numpy as jnp
from jax import lax

MODEL = 2048
HEADS = 16
HEAD = 64
GROUPS = 4
STATE = 64
KERNEL = 5
SPAN = 1024
SEQS = 8
LEN = 16384


def draw_context_input_tensor(key, part):
    key_base, key_scale = jax.random.split(jax.random.fold_in(key, 11))
    normal_part = jnp.clip(jax.random.normal(key_base, (SEQS, LEN, MODEL), jnp.float32), -4.0, 4.0)
    block_scale = jnp.exp(jax.random.uniform(key_scale, (SEQS, LEN // SPAN, 1, 1), jnp.float32, math.log(0.5), math.log(2.0)))
    shaped = normal_part.reshape(SEQS, LEN // SPAN, SPAN, MODEL) * block_scale
    return shaped.reshape(SEQS, LEN, MODEL).astype(jnp.bfloat16)


def draw_channel_fading_exponent(key, part):
    key_order, key_slow, key_fast = jax.random.split(jax.random.fold_in(key, 23), 3)
    ranking = jax.random.permutation(key_order, HEADS)
    slow_rate = jax.random.uniform(key_slow, (HEADS,), jnp.float32, 0.3, 1.5) / LEN
    fast_rate = jnp.exp(jax.random.uniform(key_fast, (HEADS,), jnp.float32, math.log(0.015), math.log(0.05)))
    fast_count = HEADS // 2
    chosen = jnp.where(ranking < fast_count, fast_rate, slow_rate)
    return jnp.log(chosen).astype(jnp.float32)


def draw_extra_damping_spikes(key, part):
    key_place, key_depth = jax.random.split(jax.random.fold_in(key, 37))
    places = jax.random.randint(key_place, (SEQS, 4), 0, LEN)
    depths = jnp.log(1.0 - jax.random.uniform(key_depth, (SEQS, 4), jnp.float32, 0.2, 0.5))
    positions = jnp.arange(LEN, dtype=jnp.int32)
    matches = (positions[None, None, :] == places[:, :, None]).astype(jnp.float32)
    summed = jnp.sum(matches * depths[:, :, None], axis=1)
    return jnp.broadcast_to(summed[:, None, :], (SEQS, HEADS, LEN)).astype(jnp.float32)


def block_levels(rng, dims, cuts, smallest, top_value):
    loudness = 1.0
    for dim, blocks in cuts:
        draws = jax.random.uniform(jax.random.fold_in(jax.random.fold_in(rng, 6), dim), (blocks,), jnp.float32, smallest / len(cuts), top_value / len(cuts))
        loudness = loudness * jnp.repeat(jnp.exp(draws), dims[dim] // blocks).reshape((-1,) + (1,) * (len(dims) - 1 - dim))
    return loudness


def normal_values(own_key, dims, scale, reach, pieces=(), kind=jnp.bfloat16):
    values = scale * jax.random.normal(own_key, dims, jnp.float32)
    if pieces:
        values = values * block_levels(own_key, dims, pieces, -0.22, 0.18)
    return jnp.clip(values, -reach, reach).astype(kind)


def setup_inputs(seed: int = 0, part: int = 0) -> dict:
    arg_keys = jax.random.split(jax.random.key(seed), 13)
    own_keys = jax.random.split(jax.random.fold_in(arg_keys[12], part), 13)
    return {
        "context_input_tensor": draw_context_input_tensor(jax.random.fold_in(jax.random.fold_in(arg_keys[12], part), 71), part),
        "content_mapping_matrix": normal_values(arg_keys[1], (MODEL, HEADS * HEAD), MODEL ** -0.5, 0.125),
        "address_mapping_matrix": normal_values(arg_keys[2], (MODEL, GROUPS * STATE), MODEL ** -0.5, 0.125),
        "increment_mapping_matrix": normal_values(arg_keys[3], (MODEL, HEADS), MODEL ** -0.5, 0.125),
        "increment_speed_offset": jnp.clip(-1.0 + 1.5 * jax.random.uniform(arg_keys[4], (HEADS,), jnp.float32) ** block_levels(arg_keys[4], (HEADS,), ((0, 16),), -0.2, 0.2), -1.0, 0.5),
        "channel_fading_exponent": draw_channel_fading_exponent(jax.random.fold_in(arg_keys[12], 71), part),
        "extra_damping_spikes": draw_extra_damping_spikes(jax.random.fold_in(jax.random.fold_in(arg_keys[12], part), 71), part),
        "content_smoothing_coefficients": normal_values(arg_keys[7], (KERNEL, HEADS, HEAD), KERNEL ** -0.5, 2.5, ((1, 16),), jnp.float32),
        "address_smoothing_coefficients": normal_values(arg_keys[8], (KERNEL, GROUPS, STATE), KERNEL ** -0.5, 2.5, (), jnp.float32),
        "newest_lookup_matrix": normal_values(own_keys[9], (SEQS, GROUPS, STATE), 1.0, 6.0, ((0, 8),)),
        "newest_output_switch": normal_values(own_keys[10], (SEQS, HEADS, HEAD), 1.0, 6.0, ((0, 8), (1, 16))),
        "cluster_scaling_coefficients": jnp.clip(1.0 + 0.18 * jax.random.normal(arg_keys[11], (HEADS, HEAD), jnp.float32), 0.1, 1.9),
    }


EPS = 1e-05

def centred(signal, kernel):
    margin = kernel.shape[0] // 2
    length = signal.shape[0]
    padded = jnp.pad(signal, ((margin, margin), (0, 0), (0, 0)))
    summed = kernel[0] * padded[0:length]
    for offset in range(1, kernel.shape[0]):
        summed = summed + kernel[offset] * padded[offset:offset + length]
    return summed

def reference(context_input_tensor, content_mapping_matrix, address_mapping_matrix, increment_mapping_matrix, increment_speed_offset, channel_fading_exponent, extra_damping_spikes, content_smoothing_coefficients, address_smoothing_coefficients, newest_lookup_matrix, newest_output_switch, cluster_scaling_coefficients):
    repeats = HEADS // GROUPS

    def lone_context_series(packed_buffer):
        prompt_token_rows, arrival_token_rows, query_vector_row, gate_vector_row = packed_buffer
        value_proj = jnp.dot(prompt_token_rows, content_mapping_matrix, preferred_element_type=jnp.float32).astype(jnp.bfloat16).reshape(LEN, HEADS, HEAD)
        key_proj = jnp.dot(prompt_token_rows, address_mapping_matrix, preferred_element_type=jnp.float32).astype(jnp.bfloat16).reshape(LEN, GROUPS, STATE)
        rate_raw = jnp.dot(prompt_token_rows, increment_mapping_matrix, preferred_element_type=jnp.float32).astype(jnp.bfloat16)
        value_conv = jax.nn.silu(centred(value_proj.astype(jnp.float32), content_smoothing_coefficients)).astype(jnp.bfloat16)
        key_conv = jax.nn.silu(centred(key_proj.astype(jnp.float32), address_smoothing_coefficients)).astype(jnp.bfloat16)
        key_heads = jnp.repeat(key_conv, repeats, axis=1)
        smoothed_increment_speed = jax.nn.softplus(rate_raw.astype(jnp.float32) + increment_speed_offset)
        exponent_increment_amount = -jnp.exp(channel_fading_exponent) * smoothed_increment_speed + arrival_token_rows.T
        cumul = jnp.cumsum(exponent_increment_amount, axis=0)
        end_weight = jnp.exp(cumul[-1] - cumul)
        weighted = (value_conv.astype(jnp.float32) * (smoothed_increment_speed * end_weight)[:, :, None]).astype(jnp.bfloat16)
        states = jnp.einsum('lhp,lhn->hpn', weighted.astype(jnp.float32), key_heads.astype(jnp.float32))
        query_heads = jnp.repeat(query_vector_row.astype(jnp.float32), repeats, axis=0)
        raw_read = jnp.einsum('hpn,hn->hp', states, query_heads, precision=lax.Precision.HIGHEST)
        gated_read = raw_read * jax.nn.silu(gate_vector_row.astype(jnp.float32))
        head_sq = lax.optimization_barrier(jnp.sum(gated_read * gated_read, axis=1))
        group_sq = jnp.repeat(lax.optimization_barrier(jnp.sum(head_sq.reshape(GROUPS, repeats), axis=1)), repeats)
        scaled = gated_read * lax.rsqrt(group_sq / (repeats * HEAD) + EPS)[:, None] * cluster_scaling_coefficients
        kv_rows = jnp.concatenate([value_conv, key_heads], axis=-1)
        return (kv_rows, scaled.astype(jnp.bfloat16))
    address_content_store, earliest_switched_retrieval = lax.map(lone_context_series, (context_input_tensor, extra_damping_spikes, newest_lookup_matrix, newest_output_switch))
    return (address_content_store, earliest_switched_retrieval)
```

```python
import functools

import jax
import jax.numpy as jnp
from jax import lax
from jax.experimental import pallas as pl
from jax.experimental.pallas import tpu as pltpu
from jax.sharding import PartitionSpec as P

HEADS = 16
HEAD = 64
GROUPS = 4
STATE = 64
KERNEL = 5
MODEL = 2048
SPAN = 1024
HALF = SPAN // 2
N = 16
Z = 4
Y = 4
LANES = 128
EPS = 1e-05
MESH = pl.DeviceIdType.MESH
CHUNK = 64


def mirror(place, side):
    return place + side * (3 - 2 * place)


def silu(v):
    return v / (1.0 + jnp.exp(-v))


def kernel(
    x_hbm,
    wv_hbm,
    wk_hbm,
    wr_hbm,
    offset_ref,
    fading_ref,
    spikes_hbm,
    vtaps_hbm,
    ktaps_hbm,
    query_hbm,
    switch_hbm,
    gain_hbm,
    kv_out,
    read_out,
    xb,
    wb,
    wr,
    spikes,
    vtaps_s,
    ktaps_s,
    query_s,
    switch_s,
    gain_s,
    acc,
    sb,
    rv,
    rk,
    notes,
    msend,
    mrecv,
    rates,
    weights,
    extv,
    extk,
    tapv,
    tapk,
    vw,
    kc,
    ob,
    states,
    qmat,
    gsend,
    grecv,
    in_sem,
    small_sem,
    k_send,
    v_send,
    f_send,
    m_send,
    k_recv,
    v_recv,
    m_recv,
    g_send,
    g_recv,
    o_sem,
):
    me = lax.axis_index("sp")
    z = me // Y
    y = me % Y
    core = lax.axis_index("tp") % 2
    side = z // 2
    zr = mirror(z, side)

    first = 3 - 2 * (1 - core) * (1 - zr)
    second = (1 - zr) * (3 - 2 * core) + 2 * zr
    third = 2 * (1 - zr)
    steps = [mirror(first, side), mirror(second, side), mirror(third, side), z]

    barrier = pltpu.get_barrier_semaphore()
    for i in range(1, N):
        pl.semaphore_signal(
            barrier, inc=1, device_id={"sp": (me + i) % N}, device_id_type=MESH
        )

    loads = []
    for i in range(4):
        rows = pl.ds(i * 256, 256)
        loads.append(pltpu.make_async_copy(x_hbm.at[rows], xb.at[rows], in_sem.at[i]))
    loads.append(pltpu.make_async_copy(wk_hbm, wb.at[0], in_sem.at[4]))
    for i in range(4):
        cols = pl.ds(pl.multiple_of(steps[i] * 256, 256), 256)
        loads.append(
            pltpu.make_async_copy(wv_hbm.at[:, cols], wb.at[i + 1], in_sem.at[5 + i])
        )
    for c in loads:
        c.start()
    smalls = [
        pltpu.make_async_copy(a, b, small_sem.at[i])
        for i, (a, b) in enumerate(
            [
                (wr_hbm, wr),
                (spikes_hbm, spikes),
                (vtaps_hbm, vtaps_s),
                (ktaps_hbm, ktaps_s),
                (query_hbm, query_s),
                (switch_hbm, switch_s),
                (gain_hbm, gain_s),
            ]
        )
    ]
    for c in smalls:
        c.start()

    def lo_mask(rows):
        return lax.broadcasted_iota(jnp.int32, (rows, LANES), 1) < HEAD

    def swap(v):
        return pltpu.roll(v, HEAD, 1)

    def remote(src, dst, ssem, rsem, peer):
        return pltpu.make_async_remote_copy(
            src_ref=src,
            dst_ref=dst,
            send_sem=ssem,
            recv_sem=rsem,
            device_id={"sp": peer},
            device_id_type=MESH,
        )

    def key_copy(zd):
        return remote(sb.at[zd], rk.at[me], k_send.at[zd], k_recv.at[me], zd * Y + y)

    def value_copy(slot, dest):
        return remote(sb.at[slot], rv.at[me], v_send.at[dest], v_recv.at[me], dest)

    def forward_copy(zs, j):
        s = zs * Y + y
        return remote(
            rk.at[s], rk.at[s], f_send.at[zs * Y + j], k_recv.at[s], z * Y + (y + j) % Y
        )

    def note_copy(dest):
        return remote(msend.at[dest], mrecv.at[me + 1], m_send.at[dest], m_recv.at[me], dest)

    notes[...] = jnp.zeros_like(notes)
    mrecv[0] = jnp.zeros((16, LANES), jnp.bfloat16)
    mrecv[N + 1] = jnp.zeros((16, LANES), jnp.bfloat16)

    for i in range(5):
        loads[i].wait()

    def tile(i, carry):
        for k in range(4):
            @pl.when(i == k + 1)
            def _():
                loads[5 + k].wait()

        acc[...] = jnp.dot(xb[...], wb[i], preferred_element_type=jnp.float32)
        low = lo_mask(CHUNK)

        def pack(c, carry2):
            r0 = pl.multiple_of(c * CHUNK, CHUNK)
            for pair in range(2):
                cols = slice(pair * LANES, (pair + 1) * LANES)
                top = acc[pl.ds(r0, CHUNK), cols]
                bot = acc[pl.ds(r0 + HALF, CHUNK), cols]
                even = jnp.where(low, top, swap(bot))
                odd = jnp.where(low, swap(top), bot)
                sb[4 * i + 2 * pair, pl.ds(r0, CHUNK)] = even.astype(jnp.bfloat16)
                sb[4 * i + 2 * pair + 1, pl.ds(r0, CHUNK)] = odd.astype(jnp.bfloat16)
            return carry2

        lax.fori_loop(0, HALF // CHUNK, pack, 0)

        low8 = lo_mask(8)
        edges = []
        for pair in range(2):
            cols = slice(pair * LANES, (pair + 1) * LANES)
            top = acc[0:8, cols]
            bot = pltpu.roll(acc[SPAN - 8 : SPAN, cols], 2, 0)
            edges.append(jnp.where(low8, bot, swap(top)))
            edges.append(jnp.where(low8, swap(bot), top))

        @pl.when(i == 0)
        def _():
            for g in range(GROUPS):
                for j in range(Y):
                    notes[g * Y + j, 10:12] = edges[g][0:2]
            pl.semaphore_wait(barrier, N - 1)
            for k in range(3):
                key_copy(steps[k]).start()

        zd = steps[0] * (i == 1) + steps[1] * (i == 2) + steps[2] * (i == 3) + z * (i == 4)

        @pl.when(i > 0)
        def _():
            for j in range(Y):
                notes[zd * Y + j, 8:10] = edges[j][0:2]

        @pl.when(jnp.logical_and(i > 0, i < 4))
        def _():
            for j in (2, 1, 3, 0):
                yd = (y + j) % Y
                value_copy(4 * i + yd, zd * Y + yd).start()

        @pl.when(i == 4)
        def _():
            for j in (2, 1, 3):
                yd = (y + j) % Y
                value_copy(16 + yd, z * Y + yd).start()

        @pl.when(i == 0)
        def _():
            rk[me] = sb[z]
            for j in (2, 1, 3):
                forward_copy(z, j).start()

        return carry

    lax.fori_loop(0, 5, tile, 0)
    rv[me] = sb[16 + y]

    for c in smalls:
        c.wait()

    raw = lax.dot_general(
        wr[...], xb[...], (((1,), (1,)), ((), ())), preferred_element_type=jnp.float32
    )
    for b in range(8):
        block = raw[:, b * LANES : (b + 1) * LANES]
        for h in range(HEADS):
            notes[h, b : b + 1] = block[h : h + 1]
    msend[...] = notes[...].astype(jnp.bfloat16)
    for i in range(1, N):
        note_copy((me + i) % N).start()
    mrecv[me + 1] = msend[me]

    for i in range(3):
        near = [1 - zr, 2 + 0 * zr, 3 + 0 * zr][i]
        zs = mirror(near, side)
        s = zs * Y + y
        remote(sb.at[0], rk.at[s], k_send.at[0], k_recv.at[s], s).wait_recv()
        for j in (2, 1, 3):
            forward_copy(zs, j).start()

    for i in range(1, N):
        s = (me + i) % N
        remote(msend.at[0], mrecv.at[s + 1], m_send.at[0], m_recv.at[s], s).wait_recv()

    for s in range(N):
        rates[8 * s : 8 * s + 8] = mrecv[s + 1].astype(jnp.float32)[0:8]
    speed = rates[...] + offset_ref[0, 0]
    speed = jnp.maximum(speed, 0.0) + jnp.log1p(jnp.exp(-jnp.abs(speed)))
    log_step = -jnp.exp(jnp.full((1, LANES), fading_ref[0, 0], jnp.float32)) * speed + spikes[...]
    ri = lax.broadcasted_iota(jnp.int32, (LANES, LANES), 0)
    ci = lax.broadcasted_iota(jnp.int32, (LANES, LANES), 1)
    later_lane = (ri > ci).astype(jnp.float32)
    later_row = (ci > ri).astype(jnp.float32)
    inner = jnp.dot(
        log_step, later_lane, precision=lax.Precision.HIGHEST, preferred_element_type=jnp.float32
    )
    outer = jnp.dot(
        later_row, log_step, precision=lax.Precision.HIGHEST, preferred_element_type=jnp.float32
    )
    suffix = inner + jnp.sum(outer, axis=1, keepdims=True)
    weights[...] = speed * jnp.exp(suffix)

    for k in range(KERNEL):
        row = vtaps_s[k : k + 1, :]
        tapv[k : k + 1, :] = jnp.concatenate([row, row], axis=1)
        row = ktaps_s[k, pl.ds(z, 1), :]
        tapk[k : k + 1, :] = jnp.concatenate([row, row], axis=1)
    qrow = query_s[...].astype(jnp.float32)
    pick = lax.broadcasted_iota(jnp.int32, (GROUPS, STATE), 0) == z
    qrow = jnp.sum(jnp.where(pick, qrow, 0.0), axis=0, keepdims=True)
    qrow = jnp.concatenate([qrow, qrow], axis=1)
    qcol = jnp.transpose(jnp.broadcast_to(qrow, (LANES, LANES)))
    qmat[...] = jnp.where((ri < STATE) == (ci < HEAD), qcol, 0.0)
    states[...] = jnp.zeros_like(states)

    def out_copy(slot, s):
        rows = pl.ds(pl.multiple_of(s * SPAN, SPAN), SPAN)
        return pltpu.make_async_copy(ob.at[slot], kv_out.at[rows], o_sem.at[slot])

    def span_of(t):
        zi = t // Y
        ji = t % Y
        zz = z * (zi == 0) + mirror(1 - zr, side) * (zi == 1)
        zz = zz + mirror(3 - zr * 0, side) * (zi == 2) + mirror(2 + zr * 0, side) * (zi == 3)
        j = 0 * (ji == 0) + 1 * (ji == 1) + 3 * (ji == 2) + 2 * (ji == 3)
        return zz * Y + (y + j) % Y, j

    low_c = lo_mask(CHUNK)

    def process(t, carry):
        s, j = span_of(t)
        slot = t % 2

        @pl.when(j != 0)
        def _():
            remote(sb.at[0], rk.at[s], k_send.at[0], k_recv.at[s], s).wait_recv()

        @pl.when(t > 0)
        def _():
            remote(sb.at[0], rv.at[s], v_send.at[0], v_recv.at[s], s).wait_recv()

        @pl.when(t >= 2)
        def _():
            out_copy(slot, s).wait()

        before = mrecv[s].astype(jnp.float32)
        after = mrecv[s + 2].astype(jnp.float32)
        low8 = lo_mask(8)
        for buf, ext, row in ((rv, extv, 8), (rk, extk, 10)):
            block = buf[s].astype(jnp.float32)
            ext[8 : 8 + HALF] = block
            head = swap(block[0:8])
            tail = swap(block[HALF - 8 : HALF])
            edge_b = before[8:16]
            edge_a = after[8:16]
            if row == 8:
                edge_b = pltpu.roll(edge_b, 6, 0)
            else:
                edge_b = pltpu.roll(edge_b, 4, 0)
                edge_a = pltpu.roll(edge_a, 6, 0)
            ext[0:8] = jnp.where(low8, edge_b, tail)
            ext[8 + HALF : 16 + HALF] = jnp.where(low8, head, edge_a)

        w8 = weights[pl.ds(pl.multiple_of(8 * s, 8), 8)]
        wcols = jnp.transpose(jnp.concatenate([w8] * 16, axis=0))
        tv = [tapv[k : k + 1, :] for k in range(KERNEL)]
        tk = [tapk[k : k + 1, :] for k in range(KERNEL)]
        for c in range(HALF // CHUNK):
            r0 = c * CHUNK
            v = tv[0] * extv[r0 + 6 : r0 + 6 + CHUNK]
            kk = tk[0] * extk[r0 + 6 : r0 + 6 + CHUNK]
            for k in range(1, KERNEL):
                v = v + tv[k] * extv[r0 + 6 + k : r0 + 6 + k + CHUNK]
                kk = kk + tk[k] * extk[r0 + 6 + k : r0 + 6 + k + CHUNK]
            v = silu(v)
            kk = silu(kk)
            b = r0 // LANES
            p0 = r0 % LANES
            wl = wcols[p0 : p0 + CHUNK, b : b + 1]
            wh = wcols[p0 : p0 + CHUNK, b + 4 : b + 5]
            w = jnp.where(low_c, wl, wh)
            vb = v.astype(jnp.bfloat16)
            vw[r0 : r0 + CHUNK] = (vb.astype(jnp.float32) * w).astype(jnp.bfloat16)
            kc[r0 : r0 + CHUNK] = kk.astype(jnp.bfloat16)
            ob[slot, r0 : r0 + CHUNK] = jnp.where(low_c, v, swap(kk)).astype(jnp.bfloat16)
            ob[slot, HALF + r0 : HALF + r0 + CHUNK] = jnp.where(low_c, swap(v), kk).astype(
                jnp.bfloat16
            )
        out_copy(slot, s).start()
        states[...] += lax.dot_general(
            kc[...], vw[...], (((0,), (0,)), ((), ())), preferred_element_type=jnp.float32
        )
        return carry

    lax.fori_loop(0, N, process, 0)

    read = jnp.sum(states[...] * qmat[...], axis=0, keepdims=True)
    read = read + swap(read)
    gate = switch_s[...].astype(jnp.float32)
    gate = jnp.concatenate([gate, gate], axis=1)
    gated = read * silu(gate)
    square = 0.5 * jnp.sum(gated * gated, axis=1, keepdims=True)
    gsend[...] = jnp.broadcast_to(square, (8, LANES))

    def square_copy(j):
        return remote(
            gsend, grecv.at[y], g_send.at[j], g_recv.at[y], z * Y + (y + j) % Y
        )

    for j in (2, 1, 3):
        square_copy(j).start()
    grecv[y] = gsend[...]
    for j in (1, 2, 3):
        yy = (y + j) % Y
        remote(gsend, grecv.at[yy], g_send.at[0], g_recv.at[yy], me).wait_recv()
    total = grecv[0] + grecv[1] + grecv[2] + grecv[3]
    gain = gain_s[...]
    gain = jnp.concatenate([gain, gain], axis=1)
    scaled = gated * lax.rsqrt(total[0:1] / (HEAD * HEADS // GROUPS) + EPS) * gain
    read_out[...] = scaled[:, :HEAD].astype(jnp.bfloat16)

    out_copy(0, 0).wait()
    out_copy(1, 0).wait()
    for j in (1, 2, 3):
        square_copy(j).wait_send()
        value_copy(16, z * Y + (y + j) % Y).wait_send()
    for k in range(3):
        key_copy(steps[k]).wait_send()
        for j in range(Y):
            value_copy(4, steps[k] * Y + j).wait_send()
    for i in range(1, N):
        note_copy((me + i) % N).wait_send()
    for zs in range(Z):
        for j in (1, 2, 3):
            forward_copy(zs, j).wait_send()


def on_device(
    context_input_tensor,
    content_mapping_matrix,
    address_mapping_matrix,
    increment_mapping_matrix,
    increment_speed_offset,
    channel_fading_exponent,
    extra_damping_spikes,
    content_smoothing_coefficients,
    address_smoothing_coefficients,
    newest_lookup_matrix,
    newest_output_switch,
    cluster_scaling_coefficients,
):
    bf16, f32 = jnp.bfloat16, jnp.float32
    anywhere = pl.BlockSpec(memory_space=pl.ANY)
    scalar = pl.BlockSpec(memory_space=pltpu.SMEM)
    dma = pltpu.SemaphoreType.DMA
    kv, read = pl.pallas_call(
        kernel,
        out_shape=(
            jax.ShapeDtypeStruct((N * SPAN, LANES), bf16),
            jax.ShapeDtypeStruct((1, HEAD), bf16),
        ),
        in_specs=[anywhere] * 4 + [scalar] * 2 + [anywhere] * 6,
        out_specs=(anywhere, pl.BlockSpec(memory_space=pltpu.VMEM)),
        scratch_shapes=[
            pltpu.VMEM((SPAN, MODEL), bf16),
            pltpu.VMEM((5, MODEL, 256), bf16),
            pltpu.VMEM((HEADS, MODEL), bf16),
            pltpu.VMEM((LANES, LANES), f32),
            pltpu.VMEM((KERNEL, HEAD), f32),
            pltpu.VMEM((KERNEL, GROUPS, STATE), f32),
            pltpu.VMEM((GROUPS, STATE), bf16),
            pltpu.VMEM((1, HEAD), bf16),
            pltpu.VMEM((1, HEAD), f32),
            pltpu.VMEM((SPAN, 256), f32),
            pltpu.VMEM((20, HALF, LANES), bf16),
            pltpu.VMEM((N, HALF, LANES), bf16),
            pltpu.VMEM((N, HALF, LANES), bf16),
            pltpu.VMEM((N, 16, LANES), f32),
            pltpu.VMEM((N, 16, LANES), bf16),
            pltpu.VMEM((N + 2, 16, LANES), bf16),
            pltpu.VMEM((LANES, LANES), f32),
            pltpu.VMEM((LANES, LANES), f32),
            pltpu.VMEM((HALF + 16, LANES), f32),
            pltpu.VMEM((HALF + 16, LANES), f32),
            pltpu.VMEM((8, LANES), f32),
            pltpu.VMEM((8, LANES), f32),
            pltpu.VMEM((HALF, LANES), bf16),
            pltpu.VMEM((HALF, LANES), bf16),
            pltpu.VMEM((2, SPAN, LANES), bf16),
            pltpu.VMEM((LANES, LANES), f32),
            pltpu.VMEM((LANES, LANES), f32),
            pltpu.VMEM((8, LANES), f32),
            pltpu.VMEM((Y, 8, LANES), f32),
            dma((9,)),
            dma((7,)),
            dma((Z,)),
            dma((N,)),
            dma((N,)),
            dma((N,)),
            dma((N,)),
            dma((N,)),
            dma((N,)),
            dma((Y,)),
            dma((Y,)),
            dma((2,)),
        ],
        compiler_params=pltpu.CompilerParams(
            collective_id=0, has_side_effects=True, vmem_limit_bytes=60 * 1024 * 1024
        ),
        name="mixer",
    )(
        context_input_tensor[0],
        content_mapping_matrix,
        address_mapping_matrix,
        increment_mapping_matrix.T,
        increment_speed_offset.reshape(1, 1),
        channel_fading_exponent.reshape(1, 1),
        extra_damping_spikes.reshape(LANES, LANES),
        content_smoothing_coefficients.reshape(KERNEL, HEAD),
        address_smoothing_coefficients,
        newest_lookup_matrix[0],
        newest_output_switch[0],
        cluster_scaling_coefficients,
    )
    return (kv.reshape(1, N * SPAN, 1, LANES), read[None])


def solution(mesh):
    placed = (
        P(("gr", "tp"), "sp", None),
        P(),
        P(),
        P(),
        P("sp"),
        P("sp"),
        P(("gr", "tp"), "sp", None),
        P(None, "sp", None),
        P(),
        P(("gr", "tp"), None, None),
        P(("gr", "tp"), "sp", None),
        P("sp", None),
    )
    return jax.shard_map(
        on_device,
        mesh=mesh,
        in_specs=placed,
        out_specs=(P(("gr", "tp"), None, "sp", None), P(("gr", "tp"), "sp", None)),
        check_vma=False,
    )
```

```python
import functools

import jax
import jax.numpy as jnp
from jax import lax
from jax.experimental import pallas as pl
from jax.experimental.pallas import tpu as pltpu
from jax.sharding import PartitionSpec as P

HEADS = 16
HEAD = 64
GROUPS = 4
STATE = 64
KERNEL = 5
MODEL = 2048
SPAN = 1024
HALF = SPAN // 2
N = 16
Z = 4
Y = 4
LANES = 128
EPS = 1e-05
MESH = pl.DeviceIdType.MESH
CHUNK = 64
NOTE = 48


def mirror(place, side):
    return place + side * (3 - 2 * place)


def silu(v):
    return v / (1.0 + jnp.exp(-v))


def kernel(
    x_hbm,
    wv_hbm,
    wk_hbm,
    wr_hbm,
    offset_ref,
    fading_ref,
    spikes_hbm,
    vtaps_hbm,
    ktaps_hbm,
    query_hbm,
    switch_hbm,
    gain_hbm,
    kv_out,
    read_out,
    xb,
    wb,
    wr,
    spikes,
    vtaps_s,
    ktaps_s,
    query_s,
    switch_s,
    gain_s,
    acc,
    sb,
    rv,
    rk,
    notes,
    nsend,
    edge_v,
    edge_k,
    rates,
    weights,
    extv,
    extk,
    tapv,
    tapk,
    vw,
    kc,
    states,
    qmat,
    gsend,
    grecv,
    in_sem,
    small_sem,
    k_send,
    n_send,
    v_send,
    f_send,
    k_recv,
    n_recv,
    v_recv,
    g_send,
    g_recv,
):
    me = lax.axis_index("sp")
    z = me // Y
    y = me % Y
    core = lax.axis_index("tp") % 2
    side = z // 2
    zr = mirror(z, side)

    first = 3 - 2 * (1 - core) * (1 - zr)
    second = (1 - zr) * (3 - 2 * core) + 2 * zr
    third = 2 * (1 - zr)
    steps = [mirror(first, side), mirror(second, side), mirror(third, side), z]

    barrier = pltpu.get_barrier_semaphore()
    for i in range(1, N):
        pl.semaphore_signal(
            barrier, inc=1, device_id={"sp": (me + i) % N}, device_id_type=MESH
        )

    loads = []
    for i in range(4):
        rows = pl.ds(i * 256, 256)
        loads.append(pltpu.make_async_copy(x_hbm.at[rows], xb.at[rows], in_sem.at[i]))
    loads.append(pltpu.make_async_copy(wk_hbm, wb.at[0], in_sem.at[4]))
    for i in range(4):
        cols = pl.ds(pl.multiple_of(steps[i] * 256, 256), 256)
        loads.append(
            pltpu.make_async_copy(wv_hbm.at[:, cols], wb.at[i + 1], in_sem.at[5 + i])
        )
    for c in loads:
        c.start()
    smalls = [
        pltpu.make_async_copy(a, b, small_sem.at[i])
        for i, (a, b) in enumerate(
            [
                (wr_hbm, wr),
                (spikes_hbm, spikes),
                (vtaps_hbm, vtaps_s),
                (ktaps_hbm, ktaps_s),
                (query_hbm, query_s),
                (switch_hbm, switch_s),
                (gain_hbm, gain_s),
            ]
        )
    ]
    for c in smalls:
        c.start()

    def lo_mask(rows):
        return lax.broadcasted_iota(jnp.int32, (rows, LANES), 1) < HEAD

    def swap(v):
        return pltpu.roll(v, HEAD, 1)

    def remote(src, dst, ssem, rsem, peer):
        return pltpu.make_async_remote_copy(
            src_ref=src,
            dst_ref=dst,
            send_sem=ssem,
            recv_sem=rsem,
            device_id={"sp": peer},
            device_id_type=MESH,
        )

    keys = pl.ds(0, HALF)
    extra = pl.ds(HALF, NOTE)

    def key_copy(zd):
        return remote(
            sb.at[zd], rk.at[me, keys], k_send.at[zd], k_recv.at[me], zd * Y + y
        )

    def note_copy(zd):
        return remote(
            nsend.at[zd], rk.at[me, extra], n_send.at[zd], n_recv.at[me], zd * Y + y
        )

    def value_copy(slot, dest):
        return remote(sb.at[slot], rv.at[me], v_send.at[dest], v_recv.at[me], dest)

    def forward_copy(zs, j):
        s = zs * Y + y
        return remote(
            rk.at[s], rk.at[s], f_send.at[zs * Y + j], k_recv.at[s], z * Y + (y + j) % Y
        )

    def multiply(i):
        acc[...] = jnp.dot(xb[...], wb[i], preferred_element_type=jnp.float32)
        low = lo_mask(CHUNK)

        def pack(c, carry2):
            r0 = pl.multiple_of(c * CHUNK, CHUNK)
            for pair in range(2):
                cols = slice(pair * LANES, (pair + 1) * LANES)
                top = acc[pl.ds(r0, CHUNK), cols]
                bot = acc[pl.ds(r0 + HALF, CHUNK), cols]
                even = jnp.where(low, top, swap(bot))
                odd = jnp.where(low, swap(top), bot)
                sb[4 * i + 2 * pair, pl.ds(r0, CHUNK)] = even.astype(jnp.bfloat16)
                sb[4 * i + 2 * pair + 1, pl.ds(r0, CHUNK)] = odd.astype(jnp.bfloat16)
            return carry2

        lax.fori_loop(0, HALF // CHUNK, pack, 0)

    low8 = lo_mask(8)

    def edge_rows(head, tail):
        out = []
        for pair in range(2):
            cols = slice(pair * LANES, (pair + 1) * LANES)
            top = head[:, cols]
            bot = pltpu.roll(tail[:, cols], 2, 0)
            out.append(jnp.where(low8, bot, swap(top))[0:2])
            out.append(jnp.where(low8, swap(bot), top)[0:2])
        return out

    notes[...] = jnp.zeros_like(notes)

    for i in range(5):
        loads[i].wait()
    multiply(0)
    pl.semaphore_wait(barrier, N - 1)
    for k in range(3):
        key_copy(steps[k]).start()
    rk[me, 0:HALF] = sb[z]

    for g, e in enumerate(edge_rows(acc[0:8], acc[SPAN - 8 : SPAN])):
        notes[g, 40:42] = e
    for c in loads[5:] + smalls:
        c.wait()
    xe = jnp.concatenate([xb[0:16], xb[SPAN - 16 : SPAN]], axis=0)
    for i in range(1, 5):
        e32 = jnp.dot(xe, wb[i], preferred_element_type=jnp.float32)
        for j, e in enumerate(edge_rows(e32[0:8], e32[24:32])):
            notes[steps[i - 1], 32 + 2 * j : 34 + 2 * j] = e
    raw = lax.dot_general(
        wr[...], xb[...], (((1,), (1,)), ((), ())), preferred_element_type=jnp.float32
    )
    for b in range(8):
        block = raw[:, b * LANES : (b + 1) * LANES]
        for h in range(HEADS):
            row = 8 * (h % Y) + b
            notes[h // Y, row : row + 1] = block[h : h + 1]
    nsend[...] = notes[...].astype(jnp.bfloat16)
    for k in range(3):
        note_copy(steps[k]).start()
    rk[me, HALF:] = nsend[z]
    for j in (2, 1, 3):
        forward_copy(z, j).start()

    def tile(i, carry):
        multiply(i)
        zd = steps[0] * (i == 1) + steps[1] * (i == 2) + steps[2] * (i == 3) + z * (i == 4)

        @pl.when(i < 4)
        def _():
            for j in (2, 1, 3, 0):
                yd = (y + j) % Y
                value_copy(4 * i + yd, zd * Y + yd).start()

        @pl.when(i == 4)
        def _():
            for j in (2, 1, 3):
                yd = (y + j) % Y
                value_copy(16 + yd, z * Y + yd).start()

        return carry

    lax.fori_loop(1, 5, tile, 0)
    rv[me] = sb[16 + y]

    for near in (1 - zr, 2 + 0 * zr, 3 + 0 * zr):
        zs = mirror(near, side)
        s = zs * Y + y
        remote(sb.at[0], rk.at[s, keys], k_send.at[0], k_recv.at[s], s).wait_recv()
        remote(nsend.at[0], rk.at[s, extra], n_send.at[0], n_recv.at[s], s).wait_recv()
        for j in (2, 1, 3):
            forward_copy(zs, j).start()
    for zz in range(Z):
        for j in (1, 2, 3):
            s = zz * Y + (y + j) % Y
            remote(rk.at[0], rk.at[s], f_send.at[0], k_recv.at[s], s).wait_recv()

    edge_v[0] = jnp.zeros((8, LANES), jnp.float32)
    edge_k[0] = jnp.zeros((8, LANES), jnp.float32)
    edge_v[N + 1] = jnp.zeros((8, LANES), jnp.float32)
    edge_k[N + 1] = jnp.zeros((8, LANES), jnp.float32)
    row8 = lax.broadcasted_iota(jnp.int32, (8, LANES), 0)

    def unpack(s, carry):
        got = rk[s, HALF:].astype(jnp.float32)
        mine = got[0:8] * (y == 0) + got[8:16] * (y == 1)
        mine = mine + got[16:24] * (y == 2) + got[24:32] * (y == 3)
        rates[pl.ds(pl.multiple_of(8 * s, 8), 8)] = mine
        ends = got[32:40]
        e0 = jnp.sum(jnp.where(row8 == 2 * y, ends, 0.0), axis=0, keepdims=True)
        e1 = jnp.sum(jnp.where(row8 == 2 * y + 1, ends, 0.0), axis=0, keepdims=True)
        even = row8 % 2 == 0
        edge_v[s + 1] = jnp.where(even, e0, e1)
        edge_k[s + 1] = jnp.where(even, got[40:41], got[41:42])
        return carry

    lax.fori_loop(0, N, unpack, 0)
    speed = rates[...] + offset_ref[0]
    speed = jnp.maximum(speed, 0.0) + jnp.log1p(jnp.exp(-jnp.abs(speed)))
    log_step = -jnp.exp(jnp.full((1, LANES), fading_ref[0], jnp.float32)) * speed + spikes[...]
    ri = lax.broadcasted_iota(jnp.int32, (LANES, LANES), 0)
    ci = lax.broadcasted_iota(jnp.int32, (LANES, LANES), 1)
    later_lane = (ri > ci).astype(jnp.float32)
    later_row = (ci > ri).astype(jnp.float32)
    inner = jnp.dot(
        log_step, later_lane, precision=lax.Precision.HIGHEST, preferred_element_type=jnp.float32
    )
    outer = jnp.dot(
        later_row, log_step, precision=lax.Precision.HIGHEST, preferred_element_type=jnp.float32
    )
    suffix = inner + jnp.sum(outer, axis=1, keepdims=True)
    weights[...] = speed * jnp.exp(suffix)

    for k in range(KERNEL):
        row = vtaps_s[k]
        tapv[k : k + 1, :] = jnp.concatenate([row, row], axis=1)
        row = ktaps_s[k, pl.ds(z, 1), :]
        tapk[k : k + 1, :] = jnp.concatenate([row, row], axis=1)
    qrow = query_s[...].astype(jnp.float32)
    pick = lax.broadcasted_iota(jnp.int32, (GROUPS, STATE), 0) == z
    qrow = jnp.sum(jnp.where(pick, qrow, 0.0), axis=0, keepdims=True)
    qrow = jnp.concatenate([qrow, qrow], axis=1)
    qcol = jnp.transpose(jnp.broadcast_to(qrow, (LANES, LANES)))
    qmat[...] = jnp.where((ri < STATE) == (ci < HEAD), qcol, 0.0)
    states[...] = jnp.zeros_like(states)

    def span_of(t):
        zi = t // Y
        ji = t % Y
        zz = z * (zi == 0) + mirror(1 - zr, side) * (zi == 1)
        zz = zz + mirror(3 - zr * 0, side) * (zi == 2) + mirror(2 + zr * 0, side) * (zi == 3)
        j = 0 * (ji == 0) + 1 * (ji == 1) + 3 * (ji == 2) + 2 * (ji == 3)
        return zz * Y + (y + j) % Y

    low_c = lo_mask(CHUNK)

    def process(t, carry):
        s = span_of(t)

        @pl.when(t > 0)
        def _():
            remote(sb.at[0], rv.at[s], v_send.at[0], v_recv.at[s], s).wait_recv()

        for buf, ext, edge in ((rv, extv, edge_v), (rk, extk, edge_k)):
            block = buf[s, 0:HALF].astype(jnp.float32)
            ext[8 : 8 + HALF] = block
            head = swap(block[0:8])
            tail = swap(block[HALF - 8 : HALF])
            ext[0:8] = jnp.where(low8, edge[s], tail)
            ext[8 + HALF : 16 + HALF] = jnp.where(low8, head, edge[s + 2])

        base = pl.multiple_of(s * SPAN, SPAN)
        w8 = weights[pl.ds(pl.multiple_of(8 * s, 8), 8)]
        wcols = jnp.transpose(jnp.concatenate([w8] * 16, axis=0))
        tv = [tapv[k : k + 1, :] for k in range(KERNEL)]
        tk = [tapk[k : k + 1, :] for k in range(KERNEL)]
        for c in range(HALF // CHUNK):
            r0 = c * CHUNK
            v = tv[0] * extv[r0 + 6 : r0 + 6 + CHUNK]
            kk = tk[0] * extk[r0 + 6 : r0 + 6 + CHUNK]
            for k in range(1, KERNEL):
                v = v + tv[k] * extv[r0 + 6 + k : r0 + 6 + k + CHUNK]
                kk = kk + tk[k] * extk[r0 + 6 + k : r0 + 6 + k + CHUNK]
            v = silu(v)
            kk = silu(kk)
            b = r0 // LANES
            p0 = r0 % LANES
            wl = wcols[p0 : p0 + CHUNK, b : b + 1]
            wh = wcols[p0 : p0 + CHUNK, b + 4 : b + 5]
            w = jnp.where(low_c, wl, wh)
            vb = v.astype(jnp.bfloat16)
            vw[r0 : r0 + CHUNK] = (vb.astype(jnp.float32) * w).astype(jnp.bfloat16)
            kc[r0 : r0 + CHUNK] = kk.astype(jnp.bfloat16)
            kv_out[pl.ds(base + r0, CHUNK)] = jnp.where(low_c, v, swap(kk)).astype(jnp.bfloat16)
            kv_out[pl.ds(base + HALF + r0, CHUNK)] = jnp.where(low_c, swap(v), kk).astype(
                jnp.bfloat16
            )
        states[...] += lax.dot_general(
            kc[...], vw[...], (((0,), (0,)), ((), ())), preferred_element_type=jnp.float32
        )
        return carry

    lax.fori_loop(0, N, process, 0)

    read = jnp.sum(states[...] * qmat[...], axis=0, keepdims=True)
    read = read + swap(read)
    gate = switch_s[...].astype(jnp.float32)
    gate = jnp.concatenate([gate, gate], axis=1)
    gated = read * silu(gate)
    square = 0.5 * jnp.sum(gated * gated, axis=1, keepdims=True)
    gsend[...] = jnp.broadcast_to(square, (8, LANES))

    def square_copy(j):
        return remote(
            gsend, grecv.at[y], g_send.at[j], g_recv.at[y], z * Y + (y + j) % Y
        )

    for j in (2, 1, 3):
        square_copy(j).start()
    grecv[y] = gsend[...]
    for j in (1, 2, 3):
        yy = (y + j) % Y
        remote(gsend, grecv.at[yy], g_send.at[0], g_recv.at[yy], me).wait_recv()
    total = grecv[0] + grecv[1] + grecv[2] + grecv[3]
    gain = gain_s[...]
    gain = jnp.concatenate([gain, gain], axis=1)
    scaled = gated * lax.rsqrt(total[0:1] / (HEAD * HEADS // GROUPS) + EPS) * gain
    read_out[...] = scaled[:, :HEAD].astype(jnp.bfloat16)

    for j in (1, 2, 3):
        square_copy(j).wait_send()
        value_copy(16, z * Y + (y + j) % Y).wait_send()
    for k in range(3):
        key_copy(steps[k]).wait_send()
        note_copy(steps[k]).wait_send()
        for j in range(Y):
            value_copy(4, steps[k] * Y + j).wait_send()
    for zs in range(Z):
        for j in (1, 2, 3):
            forward_copy(zs, j).wait_send()


def in_hbm(a):
    return pltpu.with_memory_space_constraint(a, pltpu.HBM)


def on_device(
    context_input_tensor,
    content_mapping_matrix,
    address_mapping_matrix,
    increment_mapping_matrix,
    increment_speed_offset,
    channel_fading_exponent,
    extra_damping_spikes,
    content_smoothing_coefficients,
    address_smoothing_coefficients,
    newest_lookup_matrix,
    newest_output_switch,
    cluster_scaling_coefficients,
):
    bf16, f32 = jnp.bfloat16, jnp.float32
    anywhere = pl.BlockSpec(memory_space=pltpu.HBM)
    dma = pltpu.SemaphoreType.DMA
    kv, read = pl.pallas_call(
        kernel,
        out_shape=(
            pltpu.VMEM((N * SPAN, LANES), bf16),
            jax.ShapeDtypeStruct((1, HEAD), bf16),
        ),
        in_specs=[anywhere] * 4 + [pl.BlockSpec(memory_space=pltpu.SMEM)] * 2 + [anywhere] * 6,
        out_specs=(pl.BlockSpec(memory_space=pltpu.VMEM),) * 2,
        scratch_shapes=[
            pltpu.VMEM((SPAN, MODEL), bf16),
            pltpu.VMEM((5, MODEL, 256), bf16),
            pltpu.VMEM((HEADS, MODEL), bf16),
            pltpu.VMEM((LANES, LANES), f32),
            pltpu.VMEM((KERNEL, 1, HEAD), f32),
            pltpu.VMEM((KERNEL, GROUPS, STATE), f32),
            pltpu.VMEM((GROUPS, STATE), bf16),
            pltpu.VMEM((1, HEAD), bf16),
            pltpu.VMEM((1, HEAD), f32),
            pltpu.VMEM((SPAN, 256), f32),
            pltpu.VMEM((20, HALF, LANES), bf16),
            pltpu.VMEM((N, HALF, LANES), bf16),
            pltpu.VMEM((N, HALF + NOTE, LANES), bf16),
            pltpu.VMEM((Z, NOTE, LANES), f32),
            pltpu.VMEM((Z, NOTE, LANES), bf16),
            pltpu.VMEM((N + 2, 8, LANES), f32),
            pltpu.VMEM((N + 2, 8, LANES), f32),
            pltpu.VMEM((LANES, LANES), f32),
            pltpu.VMEM((LANES, LANES), f32),
            pltpu.VMEM((HALF + 16, LANES), f32),
            pltpu.VMEM((HALF + 16, LANES), f32),
            pltpu.VMEM((8, LANES), f32),
            pltpu.VMEM((8, LANES), f32),
            pltpu.VMEM((HALF, LANES), bf16),
            pltpu.VMEM((HALF, LANES), bf16),
            pltpu.VMEM((LANES, LANES), f32),
            pltpu.VMEM((LANES, LANES), f32),
            pltpu.VMEM((8, LANES), f32),
            pltpu.VMEM((Y, 8, LANES), f32),
            dma((9,)),
            dma((7,)),
            dma((Z,)),
            dma((Z,)),
            dma((N,)),
            dma((N,)),
            dma((N,)),
            dma((N,)),
            dma((N,)),
            dma((Y,)),
            dma((Y,)),
        ],
        compiler_params=pltpu.CompilerParams(
            collective_id=0, has_side_effects=True, vmem_limit_bytes=36 * 1024 * 1024
        ),
        name="mixer",
    )(
        *map(
            in_hbm,
            (
                context_input_tensor[0],
                content_mapping_matrix,
                address_mapping_matrix,
                increment_mapping_matrix.T,
            ),
        ),
        increment_speed_offset,
        channel_fading_exponent,
        *map(
            in_hbm,
            (
                extra_damping_spikes.reshape(LANES, LANES),
                content_smoothing_coefficients,
                address_smoothing_coefficients,
                newest_lookup_matrix[0],
                newest_output_switch[0],
                cluster_scaling_coefficients,
            ),
        ),
    )
    return (kv.reshape(1, N * SPAN, 1, LANES), read[None])


def solution(mesh):
    placed = (
        P(("gr", "tp"), "sp", None),
        P(),
        P(),
        P(),
        P("sp"),
        P("sp"),
        P(("gr", "tp"), "sp", None),
        P(None, "sp", None),
        P(),
        P(("gr", "tp"), None, None),
        P(("gr", "tp"), "sp", None),
        P("sp", None),
    )
    return jax.shard_map(
        on_device,
        mesh=mesh,
        in_specs=placed,
        out_specs=(P(("gr", "tp"), None, "sp", None), P(("gr", "tp"), "sp", None)),
        check_vma=False,
    )
```

```python
import functools

import jax
import jax.numpy as jnp
from jax import lax
from jax.experimental import pallas as pl
from jax.experimental.pallas import tpu as pltpu
from jax.sharding import PartitionSpec as P

HEADS = 16
HEAD = 64
GROUPS = 4
STATE = 64
KERNEL = 5
MODEL = 2048
SPAN = 1024
HALF = SPAN // 2
N = 16
Z = 4
Y = 4
LANES = 128
EPS = 1e-05
MESH = pl.DeviceIdType.MESH
CHUNK = 64
NOTE = 48
CUT = 288


def mirror(place, side):
    return place + side * (3 - 2 * place)


def silu(v):
    return v / (1.0 + jnp.exp(-v))


def kernel(
    x_hbm,
    wv_hbm,
    wk_hbm,
    wr_hbm,
    offset_ref,
    fading_ref,
    spikes_hbm,
    vtaps_hbm,
    ktaps_hbm,
    query_hbm,
    switch_hbm,
    gain_hbm,
    kv_out,
    read_out,
    xb,
    wb,
    wr,
    spikes,
    vtaps_s,
    ktaps_s,
    query_s,
    switch_s,
    gain_s,
    acc,
    sb,
    rv,
    rk,
    notes,
    nsend,
    edge_v,
    edge_k,
    rates,
    weights,
    extv,
    extk,
    tapv,
    tapk,
    vw,
    kc,
    states,
    qmat,
    gsend,
    grecv,
    in_sem,
    small_sem,
    k_send,
    n_send,
    v_send,
    f_send,
    k_recv,
    n_recv,
    v_recv,
    g_send,
    g_recv,
):
    me = lax.axis_index("sp")
    z = me // Y
    y = me % Y
    core = lax.axis_index("tp") % 2
    side = z // 2
    zr = mirror(z, side)

    first = 3 - 2 * (1 - core) * (1 - zr)
    second = (1 - zr) * (3 - 2 * core) + 2 * zr
    third = 2 * (1 - zr)
    steps = [mirror(first, side), mirror(second, side), mirror(third, side), z]

    barrier = pltpu.get_barrier_semaphore()
    for i in range(1, N):
        pl.semaphore_signal(
            barrier, inc=1, device_id={"sp": (me + i) % N}, device_id_type=MESH
        )

    loads = []
    for i in range(4):
        rows = pl.ds(i * 256, 256)
        loads.append(pltpu.make_async_copy(x_hbm.at[rows], xb.at[rows], in_sem.at[i]))
    loads.append(pltpu.make_async_copy(wk_hbm, wb.at[0], in_sem.at[4]))
    for i in range(4):
        cols = pl.ds(pl.multiple_of(steps[i] * 256, 256), 256)
        loads.append(
            pltpu.make_async_copy(wv_hbm.at[:, cols], wb.at[i + 1], in_sem.at[5 + i])
        )
    for c in loads:
        c.start()
    smalls = [
        pltpu.make_async_copy(a, b, small_sem.at[i])
        for i, (a, b) in enumerate(
            [
                (wr_hbm, wr),
                (spikes_hbm, spikes),
                (vtaps_hbm, vtaps_s),
                (ktaps_hbm, ktaps_s),
                (query_hbm, query_s),
                (switch_hbm, switch_s),
                (gain_hbm, gain_s),
            ]
        )
    ]
    for c in smalls:
        c.start()

    def lo_mask(rows):
        return lax.broadcasted_iota(jnp.int32, (rows, LANES), 1) < HEAD

    def swap(v):
        return pltpu.roll(v, HEAD, 1)

    def remote(src, dst, ssem, rsem, peer):
        return pltpu.make_async_remote_copy(
            src_ref=src,
            dst_ref=dst,
            send_sem=ssem,
            recv_sem=rsem,
            device_id={"sp": peer},
            device_id_type=MESH,
        )

    keys = pl.ds(0, HALF)
    extra = pl.ds(HALF, NOTE)

    def key_copy(zd):
        return remote(
            sb.at[zd], rk.at[me, keys], k_send.at[zd], k_recv.at[me], zd * Y + y
        )

    def note_copy(zd):
        return remote(
            nsend.at[zd], rk.at[me, extra], n_send.at[zd], n_recv.at[me], zd * Y + y
        )

    def value_copy(slot, dest):
        return remote(sb.at[slot], rv.at[me], v_send.at[dest], v_recv.at[me], dest)

    def step_copy(zs, way):
        s = zs * Y + y
        return remote(
            rk.at[s],
            rk.at[s],
            f_send.at[zs * Y + (1 - way) // 2],
            k_recv.at[s],
            z * Y + (y + way) % Y,
        )

    def half_copy(zs, way):
        s = zs * Y + (y - way) % Y
        part = pl.ds(0, CUT) if way == 1 else pl.ds(CUT, HALF + NOTE - CUT)
        return remote(
            rk.at[s, part],
            rk.at[s, part],
            f_send.at[zs * Y + 2 + (1 - way) // 2],
            k_recv.at[s] if way == 1 else n_recv.at[s],
            z * Y + (y + way) % Y,
        )

    def multiply(i):
        acc[...] = jnp.dot(xb[...], wb[i], preferred_element_type=jnp.float32)
        low = lo_mask(CHUNK)

        def pack(c, carry2):
            r0 = pl.multiple_of(c * CHUNK, CHUNK)
            for pair in range(2):
                cols = slice(pair * LANES, (pair + 1) * LANES)
                top = acc[pl.ds(r0, CHUNK), cols]
                bot = acc[pl.ds(r0 + HALF, CHUNK), cols]
                even = jnp.where(low, top, swap(bot))
                odd = jnp.where(low, swap(top), bot)
                sb[4 * i + 2 * pair, pl.ds(r0, CHUNK)] = even.astype(jnp.bfloat16)
                sb[4 * i + 2 * pair + 1, pl.ds(r0, CHUNK)] = odd.astype(jnp.bfloat16)
            return carry2

        lax.fori_loop(0, HALF // CHUNK, pack, 0)

    low8 = lo_mask(8)

    def edge_rows(head, tail):
        out = []
        for pair in range(2):
            cols = slice(pair * LANES, (pair + 1) * LANES)
            top = head[:, cols]
            bot = pltpu.roll(tail[:, cols], 2, 0)
            out.append(jnp.where(low8, bot, swap(top))[0:2])
            out.append(jnp.where(low8, swap(bot), top)[0:2])
        return out

    notes[...] = jnp.zeros_like(notes)

    for i in range(5):
        loads[i].wait()
    multiply(0)
    pl.semaphore_wait(barrier, N - 1)
    for k in range(3):
        key_copy(steps[k]).start()
    rk[me, 0:HALF] = sb[z]

    for g, e in enumerate(edge_rows(acc[0:8], acc[SPAN - 8 : SPAN])):
        notes[g, 40:42] = e
    for c in loads[5:] + smalls:
        c.wait()
    xe = jnp.concatenate([xb[0:16], xb[SPAN - 16 : SPAN]], axis=0)
    for i in range(1, 5):
        e32 = jnp.dot(xe, wb[i], preferred_element_type=jnp.float32)
        for j, e in enumerate(edge_rows(e32[0:8], e32[24:32])):
            notes[steps[i - 1], 32 + 2 * j : 34 + 2 * j] = e
    raw = lax.dot_general(
        wr[...], xb[...], (((1,), (1,)), ((), ())), preferred_element_type=jnp.float32
    )
    for b in range(8):
        block = raw[:, b * LANES : (b + 1) * LANES]
        for h in range(HEADS):
            row = 8 * (h % Y) + b
            notes[h // Y, row : row + 1] = block[h : h + 1]
    nsend[...] = notes[...].astype(jnp.bfloat16)
    for k in range(3):
        note_copy(steps[k]).start()
    rk[me, HALF:] = nsend[z]
    for way in (1, -1):
        step_copy(z, way).start()

    def tile(i, carry):
        multiply(i)
        zd = steps[0] * (i == 1) + steps[1] * (i == 2) + steps[2] * (i == 3) + z * (i == 4)

        @pl.when(i < 4)
        def _():
            for j in (2, 1, 3, 0):
                yd = (y + j) % Y
                value_copy(4 * i + yd, zd * Y + yd).start()

        return carry

    lax.fori_loop(1, 5, tile, 0)
    rv[me] = sb[16 + y]

    def pass_on(zs):
        for way in (1, -1):
            s = zs * Y + (y - way) % Y
            remote(rk.at[0], rk.at[s], f_send.at[0], k_recv.at[s], s).wait_recv()
            half_copy(zs, way).start()

    places = [z, mirror(1 - zr, side), mirror(2 + 0 * zr, side), mirror(3 + 0 * zr, side)]
    for i in range(1, 4):
        s = places[i] * Y + y
        remote(sb.at[0], rk.at[s, keys], k_send.at[0], k_recv.at[s], s).wait_recv()
        remote(nsend.at[0], rk.at[s, extra], n_send.at[0], n_recv.at[s], s).wait_recv()
        for way in (1, -1):
            step_copy(places[i], way).start()
        pass_on(places[i - 1])
    pass_on(places[3])
    for j in (2, 1, 3):
        yd = (y + j) % Y
        value_copy(16 + yd, z * Y + yd).start()
    for zz in range(Z):
        s = zz * Y + (y + 2) % Y
        part = pl.ds(0, CUT)
        remote(rk.at[0, part], rk.at[s, part], f_send.at[0], k_recv.at[s], s).wait_recv()
        part = pl.ds(CUT, HALF + NOTE - CUT)
        remote(rk.at[0, part], rk.at[s, part], f_send.at[0], n_recv.at[s], s).wait_recv()

    edge_v[0] = jnp.zeros((8, LANES), jnp.float32)
    edge_k[0] = jnp.zeros((8, LANES), jnp.float32)
    edge_v[N + 1] = jnp.zeros((8, LANES), jnp.float32)
    edge_k[N + 1] = jnp.zeros((8, LANES), jnp.float32)
    row8 = lax.broadcasted_iota(jnp.int32, (8, LANES), 0)

    def unpack(s, carry):
        got = rk[s, HALF:].astype(jnp.float32)
        mine = got[0:8] * (y == 0) + got[8:16] * (y == 1)
        mine = mine + got[16:24] * (y == 2) + got[24:32] * (y == 3)
        rates[pl.ds(pl.multiple_of(8 * s, 8), 8)] = mine
        ends = got[32:40]
        e0 = jnp.sum(jnp.where(row8 == 2 * y, ends, 0.0), axis=0, keepdims=True)
        e1 = jnp.sum(jnp.where(row8 == 2 * y + 1, ends, 0.0), axis=0, keepdims=True)
        even = row8 % 2 == 0
        edge_v[s + 1] = jnp.where(even, e0, e1)
        edge_k[s + 1] = jnp.where(even, got[40:41], got[41:42])
        return carry

    lax.fori_loop(0, N, unpack, 0)
    speed = rates[...] + offset_ref[0]
    speed = jnp.maximum(speed, 0.0) + jnp.log1p(jnp.exp(-jnp.abs(speed)))
    log_step = -jnp.exp(jnp.full((1, LANES), fading_ref[0], jnp.float32)) * speed + spikes[...]
    ri = lax.broadcasted_iota(jnp.int32, (LANES, LANES), 0)
    ci = lax.broadcasted_iota(jnp.int32, (LANES, LANES), 1)
    later_lane = (ri > ci).astype(jnp.float32)
    later_row = (ci > ri).astype(jnp.float32)
    inner = jnp.dot(
        log_step, later_lane, precision=lax.Precision.HIGHEST, preferred_element_type=jnp.float32
    )
    outer = jnp.dot(
        later_row, log_step, precision=lax.Precision.HIGHEST, preferred_element_type=jnp.float32
    )
    suffix = inner + jnp.sum(outer, axis=1, keepdims=True)
    weights[...] = speed * jnp.exp(suffix)

    for k in range(KERNEL):
        row = vtaps_s[k]
        tapv[k : k + 1, :] = jnp.concatenate([row, row], axis=1)
        row = ktaps_s[k, pl.ds(z, 1), :]
        tapk[k : k + 1, :] = jnp.concatenate([row, row], axis=1)
    qrow = query_s[...].astype(jnp.float32)
    pick = lax.broadcasted_iota(jnp.int32, (GROUPS, STATE), 0) == z
    qrow = jnp.sum(jnp.where(pick, qrow, 0.0), axis=0, keepdims=True)
    qrow = jnp.concatenate([qrow, qrow], axis=1)
    qcol = jnp.transpose(jnp.broadcast_to(qrow, (LANES, LANES)))
    qmat[...] = jnp.where((ri < STATE) == (ci < HEAD), qcol, 0.0)
    states[...] = jnp.zeros_like(states)

    def span_of(t):
        zi = t // Y
        ji = t % Y
        place = 3 * (zi == 0) + (1 - zr) * 2 * (zi == 1) + (zi == 2) + zr * 2 * (zi == 3)
        zz = mirror(place, side)
        j = 2 * (ji == 0) + 3 * (ji == 1) + (ji == 2)
        return zz * Y + (y + j) % Y

    low_c = lo_mask(CHUNK)

    def process(t, carry):
        s = span_of(t)

        @pl.when(s != me)
        def _():
            remote(sb.at[0], rv.at[s], v_send.at[0], v_recv.at[s], s).wait_recv()

        for buf, ext, edge in ((rv, extv, edge_v), (rk, extk, edge_k)):
            block = buf[s, 0:HALF].astype(jnp.float32)
            ext[8 : 8 + HALF] = block
            head = swap(block[0:8])
            tail = swap(block[HALF - 8 : HALF])
            ext[0:8] = jnp.where(low8, edge[s], tail)
            ext[8 + HALF : 16 + HALF] = jnp.where(low8, head, edge[s + 2])

        base = pl.multiple_of(s * SPAN, SPAN)
        w8 = weights[pl.ds(pl.multiple_of(8 * s, 8), 8)]
        wcols = jnp.transpose(jnp.concatenate([w8] * 16, axis=0))
        tv = [tapv[k : k + 1, :] for k in range(KERNEL)]
        tk = [tapk[k : k + 1, :] for k in range(KERNEL)]
        for c in range(HALF // CHUNK):
            r0 = c * CHUNK
            v = tv[0] * extv[r0 + 6 : r0 + 6 + CHUNK]
            kk = tk[0] * extk[r0 + 6 : r0 + 6 + CHUNK]
            for k in range(1, KERNEL):
                v = v + tv[k] * extv[r0 + 6 + k : r0 + 6 + k + CHUNK]
                kk = kk + tk[k] * extk[r0 + 6 + k : r0 + 6 + k + CHUNK]
            v = silu(v)
            kk = silu(kk)
            b = r0 // LANES
            p0 = r0 % LANES
            wl = wcols[p0 : p0 + CHUNK, b : b + 1]
            wh = wcols[p0 : p0 + CHUNK, b + 4 : b + 5]
            w = jnp.where(low_c, wl, wh)
            vb = v.astype(jnp.bfloat16)
            vw[r0 : r0 + CHUNK] = (vb.astype(jnp.float32) * w).astype(jnp.bfloat16)
            kc[r0 : r0 + CHUNK] = kk.astype(jnp.bfloat16)
            kv_out[pl.ds(base + r0, CHUNK)] = jnp.where(low_c, v, swap(kk)).astype(jnp.bfloat16)
            kv_out[pl.ds(base + HALF + r0, CHUNK)] = jnp.where(low_c, swap(v), kk).astype(
                jnp.bfloat16
            )
        states[...] += lax.dot_general(
            kc[...], vw[...], (((0,), (0,)), ((), ())), preferred_element_type=jnp.float32
        )
        return carry

    lax.fori_loop(0, N, process, 0)

    read = jnp.sum(states[...] * qmat[...], axis=0, keepdims=True)
    read = read + swap(read)
    gate = switch_s[...].astype(jnp.float32)
    gate = jnp.concatenate([gate, gate], axis=1)
    gated = read * silu(gate)
    square = 0.5 * jnp.sum(gated * gated, axis=1, keepdims=True)
    gsend[...] = jnp.broadcast_to(square, (8, LANES))

    def square_copy(j):
        return remote(
            gsend, grecv.at[y], g_send.at[j], g_recv.at[y], z * Y + (y + j) % Y
        )

    for j in (2, 1, 3):
        square_copy(j).start()
    grecv[y] = gsend[...]
    for j in (1, 2, 3):
        yy = (y + j) % Y
        remote(gsend, grecv.at[yy], g_send.at[0], g_recv.at[yy], me).wait_recv()
    total = grecv[0] + grecv[1] + grecv[2] + grecv[3]
    gain = gain_s[...]
    gain = jnp.concatenate([gain, gain], axis=1)
    scaled = gated * lax.rsqrt(total[0:1] / (HEAD * HEADS // GROUPS) + EPS) * gain
    read_out[...] = scaled[:, :HEAD].astype(jnp.bfloat16)

    for j in (1, 2, 3):
        square_copy(j).wait_send()
        value_copy(16, z * Y + (y + j) % Y).wait_send()
    for k in range(3):
        key_copy(steps[k]).wait_send()
        note_copy(steps[k]).wait_send()
        for j in range(Y):
            value_copy(4, steps[k] * Y + j).wait_send()
    for zs in range(Z):
        for way in (1, -1):
            step_copy(zs, way).wait_send()
            half_copy(zs, way).wait_send()


def in_hbm(a):
    return pltpu.with_memory_space_constraint(a, pltpu.HBM)


def on_device(
    context_input_tensor,
    content_mapping_matrix,
    address_mapping_matrix,
    increment_mapping_matrix,
    increment_speed_offset,
    channel_fading_exponent,
    extra_damping_spikes,
    content_smoothing_coefficients,
    address_smoothing_coefficients,
    newest_lookup_matrix,
    newest_output_switch,
    cluster_scaling_coefficients,
):
    bf16, f32 = jnp.bfloat16, jnp.float32
    anywhere = pl.BlockSpec(memory_space=pltpu.HBM)
    dma = pltpu.SemaphoreType.DMA
    kv, read = pl.pallas_call(
        kernel,
        out_shape=(
            pltpu.VMEM((N * SPAN, LANES), bf16),
            jax.ShapeDtypeStruct((1, HEAD), bf16),
        ),
        in_specs=[anywhere] * 4 + [pl.BlockSpec(memory_space=pltpu.SMEM)] * 2 + [anywhere] * 6,
        out_specs=(pl.BlockSpec(memory_space=pltpu.VMEM),) * 2,
        scratch_shapes=[
            pltpu.VMEM((SPAN, MODEL), bf16),
            pltpu.VMEM((5, MODEL, 256), bf16),
            pltpu.VMEM((HEADS, MODEL), bf16),
            pltpu.VMEM((LANES, LANES), f32),
            pltpu.VMEM((KERNEL, 1, HEAD), f32),
            pltpu.VMEM((KERNEL, GROUPS, STATE), f32),
            pltpu.VMEM((GROUPS, STATE), bf16),
            pltpu.VMEM((1, HEAD), bf16),
            pltpu.VMEM((1, HEAD), f32),
            pltpu.VMEM((SPAN, 256), f32),
            pltpu.VMEM((20, HALF, LANES), bf16),
            pltpu.VMEM((N, HALF, LANES), bf16),
            pltpu.VMEM((N, HALF + NOTE, LANES), bf16),
            pltpu.VMEM((Z, NOTE, LANES), f32),
            pltpu.VMEM((Z, NOTE, LANES), bf16),
            pltpu.VMEM((N + 2, 8, LANES), f32),
            pltpu.VMEM((N + 2, 8, LANES), f32),
            pltpu.VMEM((LANES, LANES), f32),
            pltpu.VMEM((LANES, LANES), f32),
            pltpu.VMEM((HALF + 16, LANES), f32),
            pltpu.VMEM((HALF + 16, LANES), f32),
            pltpu.VMEM((8, LANES), f32),
            pltpu.VMEM((8, LANES), f32),
            pltpu.VMEM((HALF, LANES), bf16),
            pltpu.VMEM((HALF, LANES), bf16),
            pltpu.VMEM((LANES, LANES), f32),
            pltpu.VMEM((LANES, LANES), f32),
            pltpu.VMEM((8, LANES), f32),
            pltpu.VMEM((Y, 8, LANES), f32),
            dma((9,)),
            dma((7,)),
            dma((Z,)),
            dma((Z,)),
            dma((N,)),
            dma((N,)),
            dma((N,)),
            dma((N,)),
            dma((N,)),
            dma((Y,)),
            dma((Y,)),
        ],
        compiler_params=pltpu.CompilerParams(
            collective_id=0, has_side_effects=True, vmem_limit_bytes=36 * 1024 * 1024
        ),
        name="mixer",
    )(
        *map(
            in_hbm,
            (
                context_input_tensor[0],
                content_mapping_matrix,
                address_mapping_matrix,
                increment_mapping_matrix.T,
            ),
        ),
        increment_speed_offset,
        channel_fading_exponent,
        *map(
            in_hbm,
            (
                extra_damping_spikes.reshape(LANES, LANES),
                content_smoothing_coefficients,
                address_smoothing_coefficients,
                newest_lookup_matrix[0],
                newest_output_switch[0],
                cluster_scaling_coefficients,
            ),
        ),
    )
    return (kv.reshape(1, N * SPAN, 1, LANES), read[None])


def solution(mesh):
    placed = (
        P(("gr", "tp"), "sp", None),
        P(),
        P(),
        P(),
        P("sp"),
        P("sp"),
        P(("gr", "tp"), "sp", None),
        P(None, "sp", None),
        P(),
        P(("gr", "tp"), None, None),
        P(("gr", "tp"), "sp", None),
        P("sp", None),
    )
    return jax.shard_map(
        on_device,
        mesh=mesh,
        in_specs=placed,
        out_specs=(P(("gr", "tp"), None, "sp", None), P(("gr", "tp"), "sp", None)),
        check_vma=False,
    )
```

```python
import functools

import jax
import jax.numpy as jnp
from jax import lax
from jax.experimental import pallas as pl
from jax.experimental.pallas import tpu as pltpu
from jax.sharding import PartitionSpec as P

HEADS = 16
HEAD = 64
GROUPS = 4
STATE = 64
KERNEL = 5
MODEL = 2048
SPAN = 1024
HALF = SPAN // 2
N = 16
Z = 4
Y = 4
LANES = 128
EPS = 1e-05
MESH = pl.DeviceIdType.MESH
CHUNK = 64
NOTE = 48
CUT = 288


def mirror(place, side):
    return place + side * (3 - 2 * place)


def silu(v):
    return v / (1.0 + jnp.exp(-v))


def kernel(
    x_hbm,
    wv_hbm,
    wk_hbm,
    wr_hbm,
    offset_ref,
    fading_ref,
    spikes_hbm,
    vtaps_hbm,
    ktaps_hbm,
    query_hbm,
    switch_hbm,
    gain_hbm,
    kv_out,
    read_out,
    xb,
    wb,
    wr,
    spikes,
    vtaps_s,
    ktaps_s,
    query_s,
    switch_s,
    gain_s,
    acc,
    sb,
    rv,
    rk,
    notes,
    nsend,
    edge_v,
    edge_k,
    rates,
    weights,
    extv,
    extk,
    tapv,
    tapk,
    vw,
    kc,
    states,
    qmat,
    gsend,
    grecv,
    in_sem,
    small_sem,
    k_send,
    n_send,
    v_send,
    f_send,
    k_recv,
    n_recv,
    v_recv,
    g_send,
    g_recv,
):
    me = lax.axis_index("sp")
    z = me // Y
    y = me % Y
    core = lax.axis_index("tp") % 2
    side = z // 2
    zr = mirror(z, side)

    first = 3 - 2 * (1 - core) * (1 - zr)
    second = (1 - zr) * (3 - 2 * core) + 2 * zr
    third = 2 * (1 - zr)
    steps = [mirror(first, side), mirror(second, side), mirror(third, side), z]

    barrier = pltpu.get_barrier_semaphore()
    for i in range(1, N):
        pl.semaphore_signal(
            barrier, inc=1, device_id={"sp": (me + i) % N}, device_id_type=MESH
        )

    loads = []
    for i in range(4):
        rows = pl.ds(i * 256, 256)
        loads.append(pltpu.make_async_copy(x_hbm.at[rows], xb.at[rows], in_sem.at[i]))
    loads.append(pltpu.make_async_copy(wk_hbm, wb.at[0], in_sem.at[4]))
    for i in range(4):
        cols = pl.ds(pl.multiple_of(steps[i] * 256, 256), 256)
        loads.append(
            pltpu.make_async_copy(wv_hbm.at[:, cols], wb.at[i + 1], in_sem.at[5 + i])
        )
    for c in loads[:5]:
        c.start()
    smalls = [
        pltpu.make_async_copy(a, b, small_sem.at[i])
        for i, (a, b) in enumerate(
            [
                (wr_hbm, wr),
                (spikes_hbm, spikes),
                (vtaps_hbm, vtaps_s),
                (ktaps_hbm, ktaps_s),
                (query_hbm, query_s),
                (switch_hbm, switch_s),
                (gain_hbm, gain_s),
            ]
        )
    ]

    def lo_mask(rows):
        return lax.broadcasted_iota(jnp.int32, (rows, LANES), 1) < HEAD

    def swap(v):
        return pltpu.roll(v, HEAD, 1)

    def remote(src, dst, ssem, rsem, peer):
        return pltpu.make_async_remote_copy(
            src_ref=src,
            dst_ref=dst,
            send_sem=ssem,
            recv_sem=rsem,
            device_id={"sp": peer},
            device_id_type=MESH,
        )

    keys = pl.ds(0, HALF)
    extra = pl.ds(HALF, NOTE)

    def key_copy(zd):
        return remote(
            sb.at[zd], rk.at[me, keys], k_send.at[zd], k_recv.at[me], zd * Y + y
        )

    def note_copy(zd):
        return remote(
            nsend.at[zd], rk.at[me, extra], n_send.at[zd], n_recv.at[me], zd * Y + y
        )

    def value_copy(slot, dest):
        return remote(sb.at[slot], rv.at[me], v_send.at[dest], v_recv.at[me], dest)

    def step_copy(zs, way):
        s = zs * Y + y
        return remote(
            rk.at[s],
            rk.at[s],
            f_send.at[zs * Y + (1 - way) // 2],
            k_recv.at[s],
            z * Y + (y + way) % Y,
        )

    def half_copy(zs, way):
        s = zs * Y + (y - way) % Y
        part = pl.ds(0, CUT) if way == 1 else pl.ds(CUT, HALF + NOTE - CUT)
        return remote(
            rk.at[s, part],
            rk.at[s, part],
            f_send.at[zs * Y + 2 + (1 - way) // 2],
            k_recv.at[s] if way == 1 else n_recv.at[s],
            z * Y + (y + way) % Y,
        )

    def multiply(i):
        acc[...] = jnp.dot(xb[...], wb[i], preferred_element_type=jnp.float32)
        low = lo_mask(CHUNK)

        for r0 in range(0, HALF, CHUNK):
            for pair in range(2):
                cols = slice(pair * LANES, (pair + 1) * LANES)
                top = acc[r0 : r0 + CHUNK, cols]
                bot = acc[r0 + HALF : r0 + HALF + CHUNK, cols]
                even = jnp.where(low, top, swap(bot))
                odd = jnp.where(low, swap(top), bot)
                sb[4 * i + 2 * pair, r0 : r0 + CHUNK] = even.astype(jnp.bfloat16)
                sb[4 * i + 2 * pair + 1, r0 : r0 + CHUNK] = odd.astype(jnp.bfloat16)

    low8 = lo_mask(8)

    def edge_rows(head, tail):
        out = []
        for pair in range(2):
            cols = slice(pair * LANES, (pair + 1) * LANES)
            top = head[:, cols]
            bot = pltpu.roll(tail[:, cols], 2, 0)
            out.append(jnp.where(low8, bot, swap(top))[0:2])
            out.append(jnp.where(low8, swap(bot), top)[0:2])
        return out

    notes[...] = jnp.zeros_like(notes)

    for c in loads[:5]:
        c.wait()
    for c in loads[5:] + smalls:
        c.start()
    multiply(0)
    pl.semaphore_wait(barrier, N - 1)
    for k in range(3):
        key_copy(steps[k]).start()
    rk[me, 0:HALF] = sb[z]

    for g, e in enumerate(edge_rows(acc[0:8], acc[SPAN - 8 : SPAN])):
        notes[g, 40:42] = e
    for c in loads[5:] + smalls:
        c.wait()
    xe = jnp.concatenate([xb[0:16], xb[SPAN - 16 : SPAN]], axis=0)
    for i in range(1, 5):
        e32 = jnp.dot(xe, wb[i], preferred_element_type=jnp.float32)
        for j, e in enumerate(edge_rows(e32[0:8], e32[24:32])):
            notes[steps[i - 1], 32 + 2 * j : 34 + 2 * j] = e
    raw = lax.dot_general(
        wr[...], xb[...], (((1,), (1,)), ((), ())), preferred_element_type=jnp.float32
    )
    for b in range(8):
        block = raw[:, b * LANES : (b + 1) * LANES]
        for h in range(HEADS):
            row = 8 * (h % Y) + b
            notes[h // Y, row : row + 1] = block[h : h + 1]
    nsend[...] = notes[...].astype(jnp.bfloat16)
    for k in range(3):
        note_copy(steps[k]).start()
    rk[me, HALF:] = nsend[z]
    for way in (1, -1):
        step_copy(z, way).start()

    def tile(i, carry):
        multiply(i)
        zd = steps[0] * (i == 1) + steps[1] * (i == 2) + steps[2] * (i == 3) + z * (i == 4)

        @pl.when(i < 4)
        def _():
            for j in (2, 1, 3, 0):
                yd = (y + j) % Y
                value_copy(4 * i + yd, zd * Y + yd).start()

        return carry

    lax.fori_loop(1, 5, tile, 0)
    rv[me] = sb[16 + y]

    def pass_on(zs):
        for way in (1, -1):
            s = zs * Y + (y - way) % Y
            remote(rk.at[0], rk.at[s], f_send.at[0], k_recv.at[s], s).wait_recv()
            half_copy(zs, way).start()

    places = [z, mirror(1 - zr, side), mirror(2 + 0 * zr, side), mirror(3 + 0 * zr, side)]
    for i in range(1, 4):
        s = places[i] * Y + y
        remote(sb.at[0], rk.at[s, keys], k_send.at[0], k_recv.at[s], s).wait_recv()
        remote(nsend.at[0], rk.at[s, extra], n_send.at[0], n_recv.at[s], s).wait_recv()
        for way in (1, -1):
            step_copy(places[i], way).start()
        pass_on(places[i - 1])
    pass_on(places[3])
    for j in (2, 1, 3):
        yd = (y + j) % Y
        value_copy(16 + yd, z * Y + yd).start()
    for zz in range(Z):
        s = zz * Y + (y + 2) % Y
        part = pl.ds(0, CUT)
        remote(rk.at[0, part], rk.at[s, part], f_send.at[0], k_recv.at[s], s).wait_recv()
        part = pl.ds(CUT, HALF + NOTE - CUT)
        remote(rk.at[0, part], rk.at[s, part], f_send.at[0], n_recv.at[s], s).wait_recv()

    edge_v[0] = jnp.zeros((8, LANES), jnp.float32)
    edge_k[0] = jnp.zeros((8, LANES), jnp.float32)
    edge_v[N + 1] = jnp.zeros((8, LANES), jnp.float32)
    edge_k[N + 1] = jnp.zeros((8, LANES), jnp.float32)
    row8 = lax.broadcasted_iota(jnp.int32, (8, LANES), 0)

    def unpack(s, carry):
        got = rk[s, HALF:].astype(jnp.float32)
        mine = got[0:8] * (y == 0) + got[8:16] * (y == 1)
        mine = mine + got[16:24] * (y == 2) + got[24:32] * (y == 3)
        rates[pl.ds(pl.multiple_of(8 * s, 8), 8)] = mine
        ends = got[32:40]
        e0 = jnp.sum(jnp.where(row8 == 2 * y, ends, 0.0), axis=0, keepdims=True)
        e1 = jnp.sum(jnp.where(row8 == 2 * y + 1, ends, 0.0), axis=0, keepdims=True)
        even = row8 % 2 == 0
        edge_v[s + 1] = jnp.where(even, e0, e1)
        edge_k[s + 1] = jnp.where(even, got[40:41], got[41:42])
        return carry

    lax.fori_loop(0, N, unpack, 0)
    speed = rates[...] + offset_ref[0]
    speed = jnp.maximum(speed, 0.0) + jnp.log1p(jnp.exp(-jnp.abs(speed)))
    log_step = -jnp.exp(jnp.full((1, LANES), fading_ref[0], jnp.float32)) * speed + spikes[...]
    ri = lax.broadcasted_iota(jnp.int32, (LANES, LANES), 0)
    ci = lax.broadcasted_iota(jnp.int32, (LANES, LANES), 1)
    later_lane = (ri > ci).astype(jnp.float32)
    later_row = (ci > ri).astype(jnp.float32)
    inner = jnp.dot(
        log_step, later_lane, precision=lax.Precision.HIGHEST, preferred_element_type=jnp.float32
    )
    outer = jnp.dot(
        later_row, log_step, precision=lax.Precision.HIGHEST, preferred_element_type=jnp.float32
    )
    suffix = inner + jnp.sum(outer, axis=1, keepdims=True)
    weights[...] = speed * jnp.exp(suffix)

    for k in range(KERNEL):
        row = vtaps_s[k]
        tapv[k : k + 1, :] = jnp.concatenate([row, row], axis=1)
        row = ktaps_s[k, pl.ds(z, 1), :]
        tapk[k : k + 1, :] = jnp.concatenate([row, row], axis=1)
    qrow = query_s[...].astype(jnp.float32)
    pick = lax.broadcasted_iota(jnp.int32, (GROUPS, STATE), 0) == z
    qrow = jnp.sum(jnp.where(pick, qrow, 0.0), axis=0, keepdims=True)
    qrow = jnp.concatenate([qrow, qrow], axis=1)
    qcol = jnp.transpose(jnp.broadcast_to(qrow, (LANES, LANES)))
    qmat[...] = jnp.where((ri < STATE) == (ci < HEAD), qcol, 0.0)
    states[...] = jnp.zeros_like(states)

    def span_of(t):
        zi = t // Y
        ji = t % Y
        place = 3 * (zi == 0) + (1 - zr) * 2 * (zi == 1) + (zi == 2) + zr * 2 * (zi == 3)
        zz = mirror(place, side)
        j = 2 * (ji == 0) + 3 * (ji == 1) + (ji == 2)
        return zz * Y + (y + j) % Y

    low_c = lo_mask(CHUNK)

    def process(t, carry):
        s = span_of(t)

        @pl.when(s != me)
        def _():
            remote(sb.at[0], rv.at[s], v_send.at[0], v_recv.at[s], s).wait_recv()

        for buf, ext, edge in ((rv, extv, edge_v), (rk, extk, edge_k)):
            block = buf[s, 0:HALF].astype(jnp.float32)
            ext[8 : 8 + HALF] = block
            head = swap(block[0:8])
            tail = swap(block[HALF - 8 : HALF])
            ext[0:8] = jnp.where(low8, edge[s], tail)
            ext[8 + HALF : 16 + HALF] = jnp.where(low8, head, edge[s + 2])

        base = pl.multiple_of(s * SPAN, SPAN)
        w8 = weights[pl.ds(pl.multiple_of(8 * s, 8), 8)]
        wcols = jnp.transpose(jnp.concatenate([w8] * 16, axis=0))
        tv = [tapv[k : k + 1, :] for k in range(KERNEL)]
        tk = [tapk[k : k + 1, :] for k in range(KERNEL)]
        for c in range(HALF // CHUNK):
            r0 = c * CHUNK
            v = tv[0] * extv[r0 + 6 : r0 + 6 + CHUNK]
            kk = tk[0] * extk[r0 + 6 : r0 + 6 + CHUNK]
            for k in range(1, KERNEL):
                v = v + tv[k] * extv[r0 + 6 + k : r0 + 6 + k + CHUNK]
                kk = kk + tk[k] * extk[r0 + 6 + k : r0 + 6 + k + CHUNK]
            v = silu(v)
            kk = silu(kk)
            b = r0 // LANES
            p0 = r0 % LANES
            wl = wcols[p0 : p0 + CHUNK, b : b + 1]
            wh = wcols[p0 : p0 + CHUNK, b + 4 : b + 5]
            w = jnp.where(low_c, wl, wh)
            vb = v.astype(jnp.bfloat16)
            vw[r0 : r0 + CHUNK] = (vb.astype(jnp.float32) * w).astype(jnp.bfloat16)
            kc[r0 : r0 + CHUNK] = kk.astype(jnp.bfloat16)
            kv_out[pl.ds(base + r0, CHUNK)] = jnp.where(low_c, v, swap(kk)).astype(jnp.bfloat16)
            kv_out[pl.ds(base + HALF + r0, CHUNK)] = jnp.where(low_c, swap(v), kk).astype(
                jnp.bfloat16
            )
        states[...] += lax.dot_general(
            kc[...], vw[...], (((0,), (0,)), ((), ())), preferred_element_type=jnp.float32
        )
        return carry

    lax.fori_loop(0, N, process, 0)

    read = jnp.sum(states[...] * qmat[...], axis=0, keepdims=True)
    read = read + swap(read)
    gate = switch_s[...].astype(jnp.float32)
    gate = jnp.concatenate([gate, gate], axis=1)
    gated = read * silu(gate)
    square = 0.5 * jnp.sum(gated * gated, axis=1, keepdims=True)
    gsend[...] = jnp.broadcast_to(square, (8, LANES))

    def square_copy(j):
        return remote(
            gsend, grecv.at[y], g_send.at[j], g_recv.at[y], z * Y + (y + j) % Y
        )

    for j in (2, 1, 3):
        square_copy(j).start()
    grecv[y] = gsend[...]
    for j in (1, 2, 3):
        yy = (y + j) % Y
        remote(gsend, grecv.at[yy], g_send.at[0], g_recv.at[yy], me).wait_recv()
    total = grecv[0] + grecv[1] + grecv[2] + grecv[3]
    gain = gain_s[...]
    gain = jnp.concatenate([gain, gain], axis=1)
    scaled = gated * lax.rsqrt(total[0:1] / (HEAD * HEADS // GROUPS) + EPS) * gain
    read_out[...] = scaled[:, :HEAD].astype(jnp.bfloat16)

    for j in (1, 2, 3):
        square_copy(j).wait_send()
        value_copy(16, z * Y + (y + j) % Y).wait_send()
    for k in range(3):
        key_copy(steps[k]).wait_send()
        note_copy(steps[k]).wait_send()
        for j in range(Y):
            value_copy(4, steps[k] * Y + j).wait_send()
    for zs in range(Z):
        for way in (1, -1):
            step_copy(zs, way).wait_send()
            half_copy(zs, way).wait_send()


def in_hbm(a):
    return pltpu.with_memory_space_constraint(a, pltpu.HBM)


def on_device(
    context_input_tensor,
    content_mapping_matrix,
    address_mapping_matrix,
    increment_mapping_matrix,
    increment_speed_offset,
    channel_fading_exponent,
    extra_damping_spikes,
    content_smoothing_coefficients,
    address_smoothing_coefficients,
    newest_lookup_matrix,
    newest_output_switch,
    cluster_scaling_coefficients,
):
    bf16, f32 = jnp.bfloat16, jnp.float32
    anywhere = pl.BlockSpec(memory_space=pltpu.HBM)
    dma = pltpu.SemaphoreType.DMA
    kv, read = pl.pallas_call(
        kernel,
        out_shape=(
            pltpu.VMEM((N * SPAN, LANES), bf16),
            jax.ShapeDtypeStruct((1, HEAD), bf16),
        ),
        in_specs=[anywhere] * 4 + [pl.BlockSpec(memory_space=pltpu.SMEM)] * 2 + [anywhere] * 6,
        out_specs=(pl.BlockSpec(memory_space=pltpu.VMEM),) * 2,
        scratch_shapes=[
            pltpu.VMEM((SPAN, MODEL), bf16),
            pltpu.VMEM((5, MODEL, 256), bf16),
            pltpu.VMEM((HEADS, MODEL), bf16),
            pltpu.VMEM((LANES, LANES), f32),
            pltpu.VMEM((KERNEL, 1, HEAD), f32),
            pltpu.VMEM((KERNEL, GROUPS, STATE), f32),
            pltpu.VMEM((GROUPS, STATE), bf16),
            pltpu.VMEM((1, HEAD), bf16),
            pltpu.VMEM((1, HEAD), f32),
            pltpu.VMEM((SPAN, 256), f32),
            pltpu.VMEM((20, HALF, LANES), bf16),
            pltpu.VMEM((N, HALF, LANES), bf16),
            pltpu.VMEM((N, HALF + NOTE, LANES), bf16),
            pltpu.VMEM((Z, NOTE, LANES), f32),
            pltpu.VMEM((Z, NOTE, LANES), bf16),
            pltpu.VMEM((N + 2, 8, LANES), f32),
            pltpu.VMEM((N + 2, 8, LANES), f32),
            pltpu.VMEM((LANES, LANES), f32),
            pltpu.VMEM((LANES, LANES), f32),
            pltpu.VMEM((HALF + 16, LANES), f32),
            pltpu.VMEM((HALF + 16, LANES), f32),
            pltpu.VMEM((8, LANES), f32),
            pltpu.VMEM((8, LANES), f32),
            pltpu.VMEM((HALF, LANES), bf16),
            pltpu.VMEM((HALF, LANES), bf16),
            pltpu.VMEM((LANES, LANES), f32),
            pltpu.VMEM((LANES, LANES), f32),
            pltpu.VMEM((8, LANES), f32),
            pltpu.VMEM((Y, 8, LANES), f32),
            dma((9,)),
            dma((7,)),
            dma((Z,)),
            dma((Z,)),
            dma((N,)),
            dma((N,)),
            dma((N,)),
            dma((N,)),
            dma((N,)),
            dma((Y,)),
            dma((Y,)),
        ],
        compiler_params=pltpu.CompilerParams(
            collective_id=0, has_side_effects=True, vmem_limit_bytes=36 * 1024 * 1024
        ),
        name="mixer",
    )(
        *map(
            in_hbm,
            (
                context_input_tensor[0],
                content_mapping_matrix,
                address_mapping_matrix,
                increment_mapping_matrix.T,
            ),
        ),
        increment_speed_offset,
        channel_fading_exponent,
        *map(
            in_hbm,
            (
                extra_damping_spikes.reshape(LANES, LANES),
                content_smoothing_coefficients,
                address_smoothing_coefficients,
                newest_lookup_matrix[0],
                newest_output_switch[0],
                cluster_scaling_coefficients,
            ),
        ),
    )
    return (kv.reshape(1, N * SPAN, 1, LANES), read[None])


def solution(mesh):
    placed = (
        P(("gr", "tp"), "sp", None),
        P(),
        P(),
        P(),
        P("sp"),
        P("sp"),
        P(("gr", "tp"), "sp", None),
        P(None, "sp", None),
        P(),
        P(("gr", "tp"), None, None),
        P(("gr", "tp"), "sp", None),
        P("sp", None),
    )
    return jax.shard_map(
        on_device,
        mesh=mesh,
        in_specs=placed,
        out_specs=(P(("gr", "tp"), None, "sp", None), P(("gr", "tp"), "sp", None)),
        check_vma=False,
    )
```

```python
import functools

import jax
import jax.numpy as jnp
from jax import lax
from jax.experimental import pallas as pl
from jax.experimental.pallas import tpu as pltpu
from jax.sharding import PartitionSpec as P

HEADS = 16
HEAD = 64
GROUPS = 4
STATE = 64
KERNEL = 5
MODEL = 2048
SPAN = 1024
HALF = SPAN // 2
N = 16
Z = 4
Y = 4
LANES = 128
EPS = 1e-05
MESH = pl.DeviceIdType.MESH
CHUNK = 64
NOTE = 48
CUT = 288
PART = HALF // 2


def mirror(place, side):
    return place + side * (3 - 2 * place)


def silu(v):
    half = 0.5 * v
    return half + half * jnp.tanh(half)


def kernel(
    x_hbm,
    wv_hbm,
    wk_hbm,
    wr_hbm,
    offset_ref,
    fading_ref,
    spikes_hbm,
    vtaps_hbm,
    ktaps_hbm,
    query_hbm,
    switch_hbm,
    gain_hbm,
    kv_out,
    read_out,
    xb,
    wb,
    wr,
    spikes,
    vtaps_s,
    ktaps_s,
    query_s,
    switch_s,
    gain_s,
    acc,
    sb,
    rv,
    rk,
    notes,
    nsend,
    edge_v,
    edge_k,
    rates,
    weights,
    extv,
    extk,
    tapv,
    tapk,
    vw,
    kc,
    states,
    qmat,
    gsend,
    grecv,
    in_sem,
    small_sem,
    k_send,
    n_send,
    v_send,
    f_send,
    k_recv,
    n_recv,
    v_recv,
    g_send,
    g_recv,
    h_recv,
    ready,
):
    me = lax.axis_index("sp")
    z = me // Y
    y = me % Y
    core = lax.axis_index("tp") % 2
    side = z // 2
    zr = mirror(z, side)

    first = 3 - 2 * (1 - core) * (1 - zr)
    second = (1 - zr) * (3 - 2 * core) + 2 * zr
    third = 2 * (1 - zr)
    steps = [mirror(first, side), mirror(second, side), mirror(third, side), z]

    barrier = pltpu.get_barrier_semaphore()
    column = [((z + i) % Z) * Y + y for i in range(1, Z)]
    row = [z * Y + (y + i) % Y for i in range(1, Y)]
    for peer in column + row:
        pl.semaphore_signal(barrier, inc=1, device_id={"sp": peer}, device_id_type=MESH)

    loads = []
    for i in (0, 2, 1, 3):
        rows = pl.ds(i * PART, PART)
        loads.append(pltpu.make_async_copy(x_hbm.at[rows], xb.at[rows], in_sem.at[i]))
    loads.insert(0, pltpu.make_async_copy(wk_hbm, wb.at[0], in_sem.at[4]))
    for i in range(4):
        cols = pl.ds(pl.multiple_of(steps[i] * 256, 256), 256)
        loads.append(
            pltpu.make_async_copy(wv_hbm.at[:, cols], wb.at[i + 1], in_sem.at[5 + i])
        )
    for c in loads[:5]:
        c.start()
    smalls = [
        pltpu.make_async_copy(a, b, small_sem.at[i])
        for i, (a, b) in enumerate(
            [
                (wr_hbm, wr),
                (spikes_hbm, spikes),
                (vtaps_hbm, vtaps_s),
                (ktaps_hbm, ktaps_s),
                (query_hbm, query_s),
                (switch_hbm, switch_s),
                (gain_hbm, gain_s),
            ]
        )
    ]

    def lo_mask(rows):
        return lax.broadcasted_iota(jnp.int32, (rows, LANES), 1) < HEAD

    def swap(v):
        return pltpu.roll(v, HEAD, 1)

    def remote(src, dst, ssem, rsem, peer):
        return pltpu.make_async_remote_copy(
            src_ref=src,
            dst_ref=dst,
            send_sem=ssem,
            recv_sem=rsem,
            device_id={"sp": peer},
            device_id_type=MESH,
        )

    keys = (pl.ds(0, PART), pl.ds(PART, PART))
    extra = pl.ds(HALF, NOTE)

    def key_copy(zd, part):
        return remote(
            sb.at[zd, keys[part]],
            rk.at[me, keys[part]],
            k_send.at[part * Z + zd],
            (k_recv, h_recv)[part].at[me],
            zd * Y + y,
        )

    def note_copy(zd):
        return remote(
            nsend.at[zd], rk.at[me, extra], n_send.at[zd], n_recv.at[me], zd * Y + y
        )

    def value_copy(slot, dest):
        return remote(sb.at[slot], rv.at[me], v_send.at[dest], v_recv.at[me], dest)

    def step_copy(zs, way):
        s = zs * Y + y
        return remote(
            rk.at[s],
            rk.at[s],
            f_send.at[zs * Y + (1 - way) // 2],
            k_recv.at[s],
            z * Y + (y + way) % Y,
        )

    def half_copy(zs, way):
        s = zs * Y + (y - way) % Y
        part = pl.ds(0, CUT) if way == 1 else pl.ds(CUT, HALF + NOTE - CUT)
        return remote(
            rk.at[s, part],
            rk.at[s, part],
            f_send.at[zs * Y + 2 + (1 - way) // 2],
            k_recv.at[s] if way == 1 else n_recv.at[s],
            z * Y + (y + way) % Y,
        )

    def multiply(i):
        acc[...] = jnp.dot(xb[...], wb[i], preferred_element_type=jnp.float32)
        pack(i, 0, HALF)

    def pack(i, start, stop):
        low = lo_mask(CHUNK)
        for r0 in range(start, stop, CHUNK):
            for pair in range(2):
                cols = slice(pair * LANES, (pair + 1) * LANES)
                top = acc[r0 : r0 + CHUNK, cols]
                bot = acc[r0 + HALF : r0 + HALF + CHUNK, cols]
                even = jnp.where(low, top, swap(bot))
                odd = jnp.where(low, swap(top), bot)
                sb[4 * i + 2 * pair, r0 : r0 + CHUNK] = even.astype(jnp.bfloat16)
                sb[4 * i + 2 * pair + 1, r0 : r0 + CHUNK] = odd.astype(jnp.bfloat16)

    low8 = lo_mask(8)

    def edge_rows(head, tail):
        out = []
        for pair in range(2):
            cols = slice(pair * LANES, (pair + 1) * LANES)
            top = head[:, cols]
            bot = pltpu.roll(tail[:, cols], 2, 0)
            out.append(jnp.where(low8, bot, swap(top))[0:2])
            out.append(jnp.where(low8, swap(bot), top)[0:2])
        return out

    notes[...] = jnp.zeros_like(notes)

    for part in range(2):
        for c in loads[2 * part + (part > 0) : 2 * part + 3]:
            c.wait()
        if part == 1:
            for c in loads[5:] + smalls:
                c.start()
        for r0 in (PART * part, HALF + PART * part):
            acc[r0 : r0 + PART] = jnp.dot(
                xb[r0 : r0 + PART], wb[0], preferred_element_type=jnp.float32
            )
        pack(0, PART * part, PART * part + PART)
        if part == 0:
            pl.semaphore_wait(barrier, Z + Y - 2)
            for peer in column:
                pl.semaphore_signal(
                    ready.at[z], inc=1, device_id={"sp": peer}, device_id_type=MESH
                )
        for k in range(3):
            key_copy(steps[k], part).start()
    rk[me, 0:HALF] = sb[z]

    for g, e in enumerate(edge_rows(acc[0:8], acc[SPAN - 8 : SPAN])):
        notes[g, 40:42] = e
    for c in loads[5:] + smalls:
        c.wait()
    xe = jnp.concatenate([xb[0:16], xb[SPAN - 16 : SPAN]], axis=0)
    for i in range(1, 5):
        e32 = jnp.dot(xe, wb[i], preferred_element_type=jnp.float32)
        for j, e in enumerate(edge_rows(e32[0:8], e32[24:32])):
            notes[steps[i - 1], 32 + 2 * j : 34 + 2 * j] = e
    raw = lax.dot_general(
        wr[...], xb[...], (((1,), (1,)), ((), ())), preferred_element_type=jnp.float32
    )
    for b in range(8):
        block = raw[:, b * LANES : (b + 1) * LANES]
        for h in range(HEADS):
            row = 8 * (h % Y) + b
            notes[h // Y, row : row + 1] = block[h : h + 1]
    nsend[...] = notes[...].astype(jnp.bfloat16)
    for k in range(3):
        note_copy(steps[k]).start()
    rk[me, HALF:] = nsend[z]
    for way in (1, -1):
        step_copy(z, way).start()

    def tile(i, carry):
        multiply(i)
        zd = steps[0] * (i == 1) + steps[1] * (i == 2) + steps[2] * (i == 3) + z * (i == 4)

        @pl.when(i < 4)
        def _():
            pl.semaphore_wait(ready.at[zd], 1)
            for j in (2, 1, 3, 0):
                yd = (y + j) % Y
                value_copy(4 * i + yd, zd * Y + yd).start()

        return carry

    lax.fori_loop(1, 5, tile, 0)
    rv[me] = sb[16 + y]

    def pass_on(zs):
        for way in (1, -1):
            s = zs * Y + (y - way) % Y
            remote(rk.at[0], rk.at[s], f_send.at[0], k_recv.at[s], s).wait_recv()
            half_copy(zs, way).start()

    places = [z, mirror(1 - zr, side), mirror(2 + 0 * zr, side), mirror(3 + 0 * zr, side)]
    for i in range(1, 4):
        s = places[i] * Y + y
        for part, sem in ((keys[0], k_recv), (keys[1], h_recv)):
            remote(sb.at[0, part], rk.at[s, part], k_send.at[0], sem.at[s], s).wait_recv()
        remote(nsend.at[0], rk.at[s, extra], n_send.at[0], n_recv.at[s], s).wait_recv()
        for way in (1, -1):
            step_copy(places[i], way).start()
        pass_on(places[i - 1])
    pass_on(places[3])
    for j in (2, 1, 3):
        yd = (y + j) % Y
        value_copy(16 + yd, z * Y + yd).start()
    for zz in range(Z):
        s = zz * Y + (y + 2) % Y
        part = pl.ds(0, CUT)
        remote(rk.at[0, part], rk.at[s, part], f_send.at[0], k_recv.at[s], s).wait_recv()
        part = pl.ds(CUT, HALF + NOTE - CUT)
        remote(rk.at[0, part], rk.at[s, part], f_send.at[0], n_recv.at[s], s).wait_recv()

    edge_v[0] = jnp.zeros((8, LANES), jnp.float32)
    edge_k[0] = jnp.zeros((8, LANES), jnp.float32)
    edge_v[N + 1] = jnp.zeros((8, LANES), jnp.float32)
    edge_k[N + 1] = jnp.zeros((8, LANES), jnp.float32)
    row8 = lax.broadcasted_iota(jnp.int32, (8, LANES), 0)

    def unpack(s, carry):
        got = rk[s, HALF:].astype(jnp.float32)
        mine = got[0:8] * (y == 0) + got[8:16] * (y == 1)
        mine = mine + got[16:24] * (y == 2) + got[24:32] * (y == 3)
        rates[pl.ds(pl.multiple_of(8 * s, 8), 8)] = mine
        ends = got[32:40]
        e0 = jnp.sum(jnp.where(row8 == 2 * y, ends, 0.0), axis=0, keepdims=True)
        e1 = jnp.sum(jnp.where(row8 == 2 * y + 1, ends, 0.0), axis=0, keepdims=True)
        even = row8 % 2 == 0
        edge_v[s + 1] = jnp.where(even, e0, e1)
        edge_k[s + 1] = jnp.where(even, got[40:41], got[41:42])
        return carry

    lax.fori_loop(0, N, unpack, 0)
    speed = rates[...] + offset_ref[0]
    speed = jnp.maximum(speed, 0.0) + jnp.log1p(jnp.exp(-jnp.abs(speed)))
    log_step = -jnp.exp(jnp.full((1, LANES), fading_ref[0], jnp.float32)) * speed + spikes[...]
    ri = lax.broadcasted_iota(jnp.int32, (LANES, LANES), 0)
    ci = lax.broadcasted_iota(jnp.int32, (LANES, LANES), 1)
    later_lane = (ri > ci).astype(jnp.float32)
    later_row = (ci > ri).astype(jnp.float32)
    inner = jnp.dot(
        log_step, later_lane, precision=lax.Precision.HIGHEST, preferred_element_type=jnp.float32
    )
    outer = jnp.dot(
        later_row, log_step, precision=lax.Precision.HIGHEST, preferred_element_type=jnp.float32
    )
    suffix = inner + jnp.sum(outer, axis=1, keepdims=True)
    weights[...] = speed * jnp.exp(suffix)

    for k in range(KERNEL):
        row = vtaps_s[k]
        tapv[k : k + 1, :] = jnp.concatenate([row, row], axis=1)
        row = ktaps_s[k, pl.ds(z, 1), :]
        tapk[k : k + 1, :] = jnp.concatenate([row, row], axis=1)
    qrow = query_s[...].astype(jnp.float32)
    pick = lax.broadcasted_iota(jnp.int32, (GROUPS, STATE), 0) == z
    qrow = jnp.sum(jnp.where(pick, qrow, 0.0), axis=0, keepdims=True)
    qrow = jnp.concatenate([qrow, qrow], axis=1)
    qcol = jnp.transpose(jnp.broadcast_to(qrow, (LANES, LANES)))
    qmat[...] = jnp.where((ri < STATE) == (ci < HEAD), qcol, 0.0)
    states[...] = jnp.zeros_like(states)

    def span_of(t):
        zi = t // Y
        ji = t % Y
        place = 3 * (zi == 0) + (1 - zr) * 2 * (zi == 1) + (zi == 2) + zr * 2 * (zi == 3)
        zz = mirror(place, side)
        j = 2 * (ji == 0) + 3 * (ji == 1) + (ji == 2)
        return zz * Y + (y + j) % Y

    low_c = lo_mask(CHUNK)

    def extend(block, edge, s, ext):
        block = block.astype(jnp.float32)
        ext[8 : 8 + HALF] = block
        ext[0:8] = jnp.where(low8, edge[s], swap(block[HALF - 8 : HALF]))
        ext[8 + HALF : 16 + HALF] = jnp.where(low8, swap(block[0:8]), edge[s + 2])

    def convolved(ext, tap, r0):
        total = tap[0:1] * ext[r0 + 6 : r0 + 6 + CHUNK]
        for k in range(1, KERNEL):
            total = total + tap[k : k + 1] * ext[r0 + 6 + k : r0 + 6 + k + CHUNK]
        return silu(total)

    def convolve_keys(s, carry):
        extend(rk[s, 0:HALF], edge_k, s, extk)
        for r0 in range(0, HALF, CHUNK):
            kc[s, r0 : r0 + CHUNK] = convolved(extk, tapk, r0).astype(jnp.bfloat16)
        return carry

    lax.fori_loop(0, N, convolve_keys, 0)

    def write_rows(s, r0, v):
        base = pl.multiple_of(s * SPAN, SPAN) + r0
        k = kc[s, r0 : r0 + CHUNK].astype(jnp.float32)
        kv_out[pl.ds(base, CHUNK)] = jnp.where(low_c, v, swap(k)).astype(jnp.bfloat16)
        kv_out[pl.ds(base + HALF, CHUNK)] = jnp.where(low_c, swap(v), k).astype(jnp.bfloat16)

    def process(t, write):
        s = span_of(t)

        @pl.when(s != me)
        def _():
            remote(sb.at[0], rv.at[s], v_send.at[0], v_recv.at[s], s).wait_recv()

        extend(rv[s], edge_v, s, extv)
        w8 = weights[pl.ds(pl.multiple_of(8 * s, 8), 8)]
        wcols = jnp.transpose(jnp.concatenate([w8] * 16, axis=0))
        for r0 in range(0, HALF, CHUNK):
            v = convolved(extv, tapv, r0)
            b = r0 // LANES
            p0 = r0 % LANES
            wl = wcols[p0 : p0 + CHUNK, b : b + 1]
            wh = wcols[p0 : p0 + CHUNK, b + 4 : b + 5]
            vb = v.astype(jnp.bfloat16)
            w = jnp.where(low_c, wl, wh)
            vw[r0 : r0 + CHUNK] = (vb.astype(jnp.float32) * w).astype(jnp.bfloat16)
            if write:
                write_rows(s, r0, v)
            else:
                rv[s, r0 : r0 + CHUNK] = vb
        states[...] += lax.dot_general(
            kc[s], vw[...], (((0,), (0,)), ((), ())), preferred_element_type=jnp.float32
        )

    def process_step(t, carry):
        process(t, True)
        return carry

    lax.fori_loop(0, N - 1, process_step, 0)
    process(N - 1, False)

    read = jnp.sum(states[...] * qmat[...], axis=0, keepdims=True)
    read = read + swap(read)
    gate = switch_s[...].astype(jnp.float32)
    gate = jnp.concatenate([gate, gate], axis=1)
    gated = read * silu(gate)
    square = 0.5 * jnp.sum(gated * gated, axis=1, keepdims=True)
    gsend[...] = jnp.broadcast_to(square, (8, LANES))

    def square_copy(j):
        return remote(
            gsend, grecv.at[y], g_send.at[j], g_recv.at[y], z * Y + (y + j) % Y
        )

    for j in (2, 1, 3):
        square_copy(j).start()
    grecv[y] = gsend[...]
    last = span_of(N - 1)
    for r0 in range(0, HALF, CHUNK):
        write_rows(last, r0, rv[last, r0 : r0 + CHUNK].astype(jnp.float32))
    for j in (1, 2, 3):
        yy = (y + j) % Y
        remote(gsend, grecv.at[yy], g_send.at[0], g_recv.at[yy], me).wait_recv()
    total = grecv[0] + grecv[1] + grecv[2] + grecv[3]
    gain = gain_s[...]
    gain = jnp.concatenate([gain, gain], axis=1)
    scaled = gated * lax.rsqrt(total[0:1] / (HEAD * HEADS // GROUPS) + EPS) * gain
    read_out[...] = scaled[:, :HEAD].astype(jnp.bfloat16)

    for j in (1, 2, 3):
        square_copy(j).wait_send()
        value_copy(16, z * Y + (y + j) % Y).wait_send()
    for k in range(3):
        for part in range(2):
            key_copy(steps[k], part).wait_send()
        note_copy(steps[k]).wait_send()
        for j in range(Y):
            value_copy(4, steps[k] * Y + j).wait_send()
    for zs in range(Z):
        for way in (1, -1):
            step_copy(zs, way).wait_send()
            half_copy(zs, way).wait_send()


def in_hbm(a):
    return pltpu.with_memory_space_constraint(a, pltpu.HBM)


def on_device(
    context_input_tensor,
    content_mapping_matrix,
    address_mapping_matrix,
    increment_mapping_matrix,
    increment_speed_offset,
    channel_fading_exponent,
    extra_damping_spikes,
    content_smoothing_coefficients,
    address_smoothing_coefficients,
    newest_lookup_matrix,
    newest_output_switch,
    cluster_scaling_coefficients,
):
    bf16, f32 = jnp.bfloat16, jnp.float32
    anywhere = pl.BlockSpec(memory_space=pltpu.HBM)
    dma = pltpu.SemaphoreType.DMA
    kv, read = pl.pallas_call(
        kernel,
        out_shape=(
            pltpu.VMEM((N * SPAN, LANES), bf16),
            jax.ShapeDtypeStruct((1, HEAD), bf16),
        ),
        in_specs=[anywhere] * 4 + [pl.BlockSpec(memory_space=pltpu.SMEM)] * 2 + [anywhere] * 6,
        out_specs=(pl.BlockSpec(memory_space=pltpu.VMEM),) * 2,
        scratch_shapes=[
            pltpu.VMEM((SPAN, MODEL), bf16),
            pltpu.VMEM((5, MODEL, 256), bf16),
            pltpu.VMEM((HEADS, MODEL), bf16),
            pltpu.VMEM((LANES, LANES), f32),
            pltpu.VMEM((KERNEL, 1, HEAD), f32),
            pltpu.VMEM((KERNEL, GROUPS, STATE), f32),
            pltpu.VMEM((GROUPS, STATE), bf16),
            pltpu.VMEM((1, HEAD), bf16),
            pltpu.VMEM((1, HEAD), f32),
            pltpu.VMEM((SPAN, 256), f32),
            pltpu.VMEM((20, HALF, LANES), bf16),
            pltpu.VMEM((N, HALF, LANES), bf16),
            pltpu.VMEM((N, HALF + NOTE, LANES), bf16),
            pltpu.VMEM((Z, NOTE, LANES), f32),
            pltpu.VMEM((Z, NOTE, LANES), bf16),
            pltpu.VMEM((N + 2, 8, LANES), f32),
            pltpu.VMEM((N + 2, 8, LANES), f32),
            pltpu.VMEM((LANES, LANES), f32),
            pltpu.VMEM((LANES, LANES), f32),
            pltpu.VMEM((HALF + 16, LANES), f32),
            pltpu.VMEM((HALF + 16, LANES), f32),
            pltpu.VMEM((8, LANES), f32),
            pltpu.VMEM((8, LANES), f32),
            pltpu.VMEM((HALF, LANES), bf16),
            pltpu.VMEM((N, HALF, LANES), bf16),
            pltpu.VMEM((LANES, LANES), f32),
            pltpu.VMEM((LANES, LANES), f32),
            pltpu.VMEM((8, LANES), f32),
            pltpu.VMEM((Y, 8, LANES), f32),
            dma((9,)),
            dma((7,)),
            dma((2 * Z,)),
            dma((Z,)),
            dma((N,)),
            dma((N,)),
            dma((N,)),
            dma((N,)),
            dma((N,)),
            dma((Y,)),
            dma((Y,)),
            dma((N,)),
            pltpu.SemaphoreType.REGULAR((Z,)),
        ],
        compiler_params=pltpu.CompilerParams(
            collective_id=0, has_side_effects=True, vmem_limit_bytes=36 * 1024 * 1024
        ),
        name="mixer",
    )(
        *map(
            in_hbm,
            (
                context_input_tensor[0],
                content_mapping_matrix,
                address_mapping_matrix,
                increment_mapping_matrix.T,
            ),
        ),
        increment_speed_offset,
        channel_fading_exponent,
        *map(
            in_hbm,
            (
                extra_damping_spikes.reshape(LANES, LANES),
                content_smoothing_coefficients,
                address_smoothing_coefficients,
                newest_lookup_matrix[0],
                newest_output_switch[0],
                cluster_scaling_coefficients,
            ),
        ),
    )
    return (kv.reshape(1, N * SPAN, 1, LANES), read[None])


def solution(mesh):
    placed = (
        P(("gr", "tp"), "sp", None),
        P(),
        P(),
        P(),
        P("sp"),
        P("sp"),
        P(("gr", "tp"), "sp", None),
        P(None, "sp", None),
        P(),
        P(("gr", "tp"), None, None),
        P(("gr", "tp"), "sp", None),
        P("sp", None),
    )
    return jax.shard_map(
        on_device,
        mesh=mesh,
        in_specs=placed,
        out_specs=(P(("gr", "tp"), None, "sp", None), P(("gr", "tp"), "sp", None)),
        check_vma=False,
    )
```

```python
import functools

import jax
import jax.numpy as jnp
from jax import lax
from jax.experimental import pallas as pl
from jax.experimental.pallas import tpu as pltpu
from jax.sharding import PartitionSpec as P

HEADS = 16
HEAD = 64
GROUPS = 4
STATE = 64
KERNEL = 5
MODEL = 2048
SPAN = 1024
HALF = SPAN // 2
N = 16
Z = 4
Y = 4
LANES = 128
EPS = 1e-05
MESH = pl.DeviceIdType.MESH
CHUNK = 64
NOTE = 48
CUT = 288
PART = HALF // 2


def mirror(place, side):
    return place + side * (3 - 2 * place)


def silu(v):
    half = 0.5 * v
    return half + half * jnp.tanh(half)


def kernel(
    x_hbm,
    wv_hbm,
    wk_hbm,
    wr_hbm,
    offset_ref,
    fading_ref,
    spikes_hbm,
    vtaps_hbm,
    ktaps_hbm,
    query_hbm,
    switch_hbm,
    gain_hbm,
    kv_out,
    read_out,
    xb,
    wb,
    wr,
    spikes,
    vtaps_s,
    ktaps_s,
    query_s,
    switch_s,
    gain_s,
    acc,
    sb,
    rv,
    rk,
    notes,
    nsend,
    edge_v,
    edge_k,
    rates,
    weights,
    chooser,
    spread,
    extv,
    extk,
    tapv,
    tapk,
    vw,
    kc,
    states,
    qmat,
    gsend,
    grecv,
    in_sem,
    small_sem,
    k_send,
    n_send,
    v_send,
    f_send,
    k_recv,
    n_recv,
    v_recv,
    g_send,
    g_recv,
    h_recv,
    ready,
):
    me = lax.axis_index("sp")
    z = me // Y
    y = me % Y
    core = lax.axis_index("tp") % 2
    side = z // 2
    zr = mirror(z, side)

    first = 3 - 2 * (1 - core) * (1 - zr)
    second = (1 - zr) * (3 - 2 * core) + 2 * zr
    third = 2 * (1 - zr)
    steps = [mirror(first, side), mirror(second, side), mirror(third, side), z]

    barrier = pltpu.get_barrier_semaphore()
    column = [((z + i) % Z) * Y + y for i in range(1, Z)]
    row = [z * Y + (y + i) % Y for i in range(1, Y)]
    for peer in column + row:
        pl.semaphore_signal(barrier, inc=1, device_id={"sp": peer}, device_id_type=MESH)

    loads = []
    for i in (0, 2, 1, 3):
        rows = pl.ds(i * PART, PART)
        loads.append(pltpu.make_async_copy(x_hbm.at[rows], xb.at[rows], in_sem.at[i]))
    loads.insert(0, pltpu.make_async_copy(wk_hbm, wb.at[0], in_sem.at[4]))
    for i in range(4):
        cols = pl.ds(pl.multiple_of(steps[i] * 256, 256), 256)
        loads.append(
            pltpu.make_async_copy(wv_hbm.at[:, cols], wb.at[i + 1], in_sem.at[5 + i])
        )
    for c in loads[:5]:
        c.start()
    smalls = [
        pltpu.make_async_copy(a, b, small_sem.at[i])
        for i, (a, b) in enumerate(
            [
                (wr_hbm, wr),
                (spikes_hbm, spikes),
                (vtaps_hbm, vtaps_s),
                (ktaps_hbm, ktaps_s),
                (query_hbm, query_s),
                (switch_hbm, switch_s),
                (gain_hbm, gain_s),
            ]
        )
    ]

    def lo_mask(rows):
        return lax.broadcasted_iota(jnp.int32, (rows, LANES), 1) < HEAD

    def swap(v):
        return pltpu.roll(v, HEAD, 1)

    def remote(src, dst, ssem, rsem, peer):
        return pltpu.make_async_remote_copy(
            src_ref=src,
            dst_ref=dst,
            send_sem=ssem,
            recv_sem=rsem,
            device_id={"sp": peer},
            device_id_type=MESH,
        )

    keys = (pl.ds(0, PART), pl.ds(PART, PART))
    extra = pl.ds(HALF, NOTE)

    def key_copy(zd, part):
        return remote(
            sb.at[zd, keys[part]],
            rk.at[me, keys[part]],
            k_send.at[part * Z + zd],
            (k_recv, h_recv)[part].at[me],
            zd * Y + y,
        )

    def note_copy(zd):
        return remote(
            nsend.at[zd], rk.at[me, extra], n_send.at[zd], n_recv.at[me], zd * Y + y
        )

    def value_copy(slot, dest):
        return remote(sb.at[slot], rv.at[me], v_send.at[dest], v_recv.at[me], dest)

    def step_copy(zs, way):
        s = zs * Y + y
        return remote(
            rk.at[s],
            rk.at[s],
            f_send.at[zs * Y + (1 - way) // 2],
            k_recv.at[s],
            z * Y + (y + way) % Y,
        )

    def half_copy(zs, way):
        s = zs * Y + (y - way) % Y
        part = pl.ds(0, CUT) if way == 1 else pl.ds(CUT, HALF + NOTE - CUT)
        return remote(
            rk.at[s, part],
            rk.at[s, part],
            f_send.at[zs * Y + 2 + (1 - way) // 2],
            k_recv.at[s] if way == 1 else n_recv.at[s],
            z * Y + (y + way) % Y,
        )

    def multiply(i):
        acc[...] = jnp.dot(xb[...], wb[i], preferred_element_type=jnp.float32)
        pack(i, 0, HALF)

    def pack(i, start, stop):
        low = lo_mask(CHUNK)
        for r0 in range(start, stop, CHUNK):
            for pair in range(2):
                cols = slice(pair * LANES, (pair + 1) * LANES)
                top = acc[r0 : r0 + CHUNK, cols]
                bot = acc[r0 + HALF : r0 + HALF + CHUNK, cols]
                even = jnp.where(low, top, swap(bot))
                odd = jnp.where(low, swap(top), bot)
                sb[4 * i + 2 * pair, r0 : r0 + CHUNK] = even.astype(jnp.bfloat16)
                sb[4 * i + 2 * pair + 1, r0 : r0 + CHUNK] = odd.astype(jnp.bfloat16)

    low8 = lo_mask(8)

    def edge_rows(head, tail):
        out = []
        for pair in range(2):
            cols = slice(pair * LANES, (pair + 1) * LANES)
            top = head[:, cols]
            bot = pltpu.roll(tail[:, cols], 2, 0)
            out.append(jnp.where(low8, bot, swap(top))[0:2])
            out.append(jnp.where(low8, swap(bot), top)[0:2])
        return out

    notes[...] = jnp.zeros_like(notes)

    for part in range(2):
        for c in loads[2 * part + (part > 0) : 2 * part + 3]:
            c.wait()
        if part == 1:
            for c in loads[5:] + smalls:
                c.start()
        for r0 in (PART * part, HALF + PART * part):
            acc[r0 : r0 + PART] = jnp.dot(
                xb[r0 : r0 + PART], wb[0], preferred_element_type=jnp.float32
            )
        pack(0, PART * part, PART * part + PART)
        if part == 0:
            pl.semaphore_wait(barrier, Z + Y - 2)
            for peer in column:
                pl.semaphore_signal(
                    ready.at[z], inc=1, device_id={"sp": peer}, device_id_type=MESH
                )
        for k in range(3):
            key_copy(steps[k], part).start()
    rk[me, 0:HALF] = sb[z]

    for g, e in enumerate(edge_rows(acc[0:8], acc[SPAN - 8 : SPAN])):
        notes[g, 40:42] = e
    for c in loads[5:] + smalls:
        c.wait()
    xe = jnp.concatenate([xb[0:16], xb[SPAN - 16 : SPAN]], axis=0)
    for i in range(1, 5):
        e32 = jnp.dot(xe, wb[i], preferred_element_type=jnp.float32)
        for j, e in enumerate(edge_rows(e32[0:8], e32[24:32])):
            notes[steps[i - 1], 32 + 2 * j : 34 + 2 * j] = e
    raw = lax.dot_general(
        wr[...], xb[...], (((1,), (1,)), ((), ())), preferred_element_type=jnp.float32
    )
    for b in range(8):
        block = raw[:, b * LANES : (b + 1) * LANES]
        for h in range(HEADS):
            row = 8 * (h % Y) + b
            notes[h // Y, row : row + 1] = block[h : h + 1]
    nsend[...] = notes[...].astype(jnp.bfloat16)
    for k in range(3):
        note_copy(steps[k]).start()
    rk[me, HALF:] = nsend[z]
    for way in (1, -1):
        step_copy(z, way).start()

    def tile(i, carry):
        multiply(i)
        zd = steps[0] * (i == 1) + steps[1] * (i == 2) + steps[2] * (i == 3) + z * (i == 4)

        @pl.when(i < 4)
        def _():
            pl.semaphore_wait(ready.at[zd], 1)
            for j in (2, 1, 3, 0):
                yd = (y + j) % Y
                value_copy(4 * i + yd, zd * Y + yd).start()

        return carry

    lax.fori_loop(1, 5, tile, 0)
    rv[me] = sb[16 + y]

    def pass_on(zs):
        for way in (1, -1):
            s = zs * Y + (y - way) % Y
            remote(rk.at[0], rk.at[s], f_send.at[0], k_recv.at[s], s).wait_recv()
            half_copy(zs, way).start()

    places = [z, mirror(1 - zr, side), mirror(2 + 0 * zr, side), mirror(3 + 0 * zr, side)]
    for i in range(1, 4):
        s = places[i] * Y + y
        for part, sem in ((keys[0], k_recv), (keys[1], h_recv)):
            remote(sb.at[0, part], rk.at[s, part], k_send.at[0], sem.at[s], s).wait_recv()
        remote(nsend.at[0], rk.at[s, extra], n_send.at[0], n_recv.at[s], s).wait_recv()
        for way in (1, -1):
            step_copy(places[i], way).start()
        pass_on(places[i - 1])
    pass_on(places[3])
    for j in (2, 1, 3):
        yd = (y + j) % Y
        value_copy(16 + yd, z * Y + yd).start()
    for zz in range(Z):
        s = zz * Y + (y + 2) % Y
        part = pl.ds(0, CUT)
        remote(rk.at[0, part], rk.at[s, part], f_send.at[0], k_recv.at[s], s).wait_recv()
        part = pl.ds(CUT, HALF + NOTE - CUT)
        remote(rk.at[0, part], rk.at[s, part], f_send.at[0], n_recv.at[s], s).wait_recv()

    edge_v[0] = jnp.zeros((8, LANES), jnp.float32)
    edge_k[0] = jnp.zeros((8, LANES), jnp.float32)
    edge_v[N + 1] = jnp.zeros((8, LANES), jnp.float32)
    edge_k[N + 1] = jnp.zeros((8, LANES), jnp.float32)
    row8 = lax.broadcasted_iota(jnp.int32, (8, LANES), 0)

    def unpack(s, carry):
        got = rk[s, HALF:].astype(jnp.float32)
        mine = got[0:8] * (y == 0) + got[8:16] * (y == 1)
        mine = mine + got[16:24] * (y == 2) + got[24:32] * (y == 3)
        rates[pl.ds(pl.multiple_of(8 * s, 8), 8)] = mine
        ends = got[32:40]
        e0 = jnp.sum(jnp.where(row8 == 2 * y, ends, 0.0), axis=0, keepdims=True)
        e1 = jnp.sum(jnp.where(row8 == 2 * y + 1, ends, 0.0), axis=0, keepdims=True)
        even = row8 % 2 == 0
        edge_v[s + 1] = jnp.where(even, e0, e1)
        edge_k[s + 1] = jnp.where(even, got[40:41], got[41:42])
        return carry

    lax.fori_loop(0, N, unpack, 0, unroll=4)
    speed = rates[...] + offset_ref[0]
    speed = jnp.maximum(speed, 0.0) + jnp.log1p(jnp.exp(-jnp.abs(speed)))
    log_step = -jnp.exp(jnp.full((1, LANES), fading_ref[0], jnp.float32)) * speed + spikes[...]
    ri = lax.broadcasted_iota(jnp.int32, (LANES, LANES), 0)
    ci = lax.broadcasted_iota(jnp.int32, (LANES, LANES), 1)
    later_lane = (ri > ci).astype(jnp.float32)
    later_row = (ci > ri).astype(jnp.float32)
    inner = jnp.dot(
        log_step, later_lane, precision=lax.Precision.HIGHEST, preferred_element_type=jnp.float32
    )
    outer = jnp.dot(
        later_row, log_step, precision=lax.Precision.HIGHEST, preferred_element_type=jnp.float32
    )
    suffix = inner + jnp.sum(outer, axis=1, keepdims=True)
    weight = speed * jnp.exp(suffix)
    for part in range(3):
        piece = weight.astype(jnp.bfloat16).astype(jnp.float32)
        weight = weight - piece
        for s in range(N):
            weights[24 * s + 8 * part : 24 * s + 8 * part + 8] = piece[8 * s : 8 * s + 8]
    shape = (24, HALF)
    wanted = lax.broadcasted_iota(jnp.int32, shape, 1)
    wanted = wanted // LANES + Y * (wanted % LANES >= HEAD)
    pick = lax.broadcasted_iota(jnp.int32, shape, 0) % 8 == wanted
    chooser[...] = pick.astype(jnp.float32).astype(jnp.bfloat16)

    for k in range(KERNEL):
        row = vtaps_s[k]
        tapv[k : k + 1, :] = jnp.concatenate([row, row], axis=1)
        row = ktaps_s[k, pl.ds(z, 1), :]
        tapk[k : k + 1, :] = jnp.concatenate([row, row], axis=1)
    qrow = query_s[...].astype(jnp.float32)
    pick = lax.broadcasted_iota(jnp.int32, (GROUPS, STATE), 0) == z
    qrow = jnp.sum(jnp.where(pick, qrow, 0.0), axis=0, keepdims=True)
    qrow = jnp.concatenate([qrow, qrow], axis=1)
    qcol = jnp.transpose(jnp.broadcast_to(qrow, (LANES, LANES)))
    qmat[...] = jnp.where((ri < STATE) == (ci < HEAD), qcol, 0.0)
    states[...] = jnp.zeros_like(states)

    def span_of(t):
        zi = t // Y
        ji = t % Y
        place = 3 * (zi == 0) + (1 - zr) * 2 * (zi == 1) + (zi == 2) + zr * 2 * (zi == 3)
        zz = mirror(place, side)
        j = 2 * (ji == 0) + 3 * (ji == 1) + (ji == 2)
        return zz * Y + (y + j) % Y

    low_c = lo_mask(CHUNK)

    def extend(block, edge, s, ext):
        block = block.astype(jnp.float32)
        ext[8 : 8 + HALF] = block
        ext[0:8] = jnp.where(low8, edge[s], swap(block[HALF - 8 : HALF]))
        ext[8 + HALF : 16 + HALF] = jnp.where(low8, swap(block[0:8]), edge[s + 2])

    def convolved(ext, tap, r0):
        total = tap[0:1] * ext[r0 + 6 : r0 + 6 + CHUNK]
        for k in range(1, KERNEL):
            total = total + tap[k : k + 1] * ext[r0 + 6 + k : r0 + 6 + k + CHUNK]
        return silu(total)

    def convolve_keys(s, carry):
        extend(rk[s, 0:HALF], edge_k, s, extk)
        for r0 in range(0, HALF, CHUNK):
            kc[s, r0 : r0 + CHUNK] = convolved(extk, tapk, r0).astype(jnp.bfloat16)
        return carry

    lax.fori_loop(0, N, convolve_keys, 0)

    def write_rows(s, r0, v):
        base = pl.multiple_of(s * SPAN, SPAN) + r0
        k = kc[s, r0 : r0 + CHUNK].astype(jnp.float32)
        kv_out[pl.ds(base, CHUNK)] = jnp.where(low_c, v, swap(k)).astype(jnp.bfloat16)
        kv_out[pl.ds(base + HALF, CHUNK)] = jnp.where(low_c, swap(v), k).astype(jnp.bfloat16)

    def process(t, write):
        s = span_of(t)

        @pl.when(s != me)
        def _():
            remote(sb.at[0], rv.at[s], v_send.at[0], v_recv.at[s], s).wait_recv()

        extend(rv[s], edge_v, s, extv)
        parts = weights[pl.ds(pl.multiple_of(24 * s, 8), 24)].astype(jnp.bfloat16)
        spread[...] = lax.dot_general(
            parts, chooser[...], (((0,), (0,)), ((), ())), preferred_element_type=jnp.float32
        )
        for r0 in range(0, HALF, CHUNK):
            v = convolved(extv, tapv, r0)
            b = r0 // LANES
            p0 = r0 % LANES
            w = spread[p0 : p0 + CHUNK, b * LANES : (b + 1) * LANES]
            vw[r0 : r0 + CHUNK] = (v * w).astype(jnp.bfloat16)
            if write:
                write_rows(s, r0, v)
            else:
                rv[s, r0 : r0 + CHUNK] = v.astype(jnp.bfloat16)
        states[...] += lax.dot_general(
            kc[s], vw[...], (((0,), (0,)), ((), ())), preferred_element_type=jnp.float32
        )

    def process_step(t, carry):
        process(t, True)
        return carry

    lax.fori_loop(0, N - 1, process_step, 0)
    process(N - 1, False)

    read = jnp.sum(states[...] * qmat[...], axis=0, keepdims=True)
    read = read + swap(read)
    gate = switch_s[...].astype(jnp.float32)
    gate = jnp.concatenate([gate, gate], axis=1)
    gated = read * silu(gate)
    square = 0.5 * jnp.sum(gated * gated, axis=1, keepdims=True)
    gsend[...] = jnp.broadcast_to(square, (8, LANES))

    def square_copy(j):
        return remote(
            gsend, grecv.at[y], g_send.at[j], g_recv.at[y], z * Y + (y + j) % Y
        )

    for j in (2, 1, 3):
        square_copy(j).start()
    grecv[y] = gsend[...]
    last = span_of(N - 1)
    for r0 in range(0, HALF, CHUNK):
        write_rows(last, r0, rv[last, r0 : r0 + CHUNK].astype(jnp.float32))
    for j in (1, 2, 3):
        yy = (y + j) % Y
        remote(gsend, grecv.at[yy], g_send.at[0], g_recv.at[yy], me).wait_recv()
    total = grecv[0] + grecv[1] + grecv[2] + grecv[3]
    gain = gain_s[...]
    gain = jnp.concatenate([gain, gain], axis=1)
    scaled = gated * lax.rsqrt(total[0:1] / (HEAD * HEADS // GROUPS) + EPS) * gain
    read_out[...] = scaled[:, :HEAD].astype(jnp.bfloat16)

    for j in (1, 2, 3):
        square_copy(j).wait_send()
        value_copy(16, z * Y + (y + j) % Y).wait_send()
    for k in range(3):
        for part in range(2):
            key_copy(steps[k], part).wait_send()
        note_copy(steps[k]).wait_send()
        for j in range(Y):
            value_copy(4, steps[k] * Y + j).wait_send()
    for zs in range(Z):
        for way in (1, -1):
            step_copy(zs, way).wait_send()
            half_copy(zs, way).wait_send()


def in_hbm(a):
    return pltpu.with_memory_space_constraint(a, pltpu.HBM)


def on_device(
    context_input_tensor,
    content_mapping_matrix,
    address_mapping_matrix,
    increment_mapping_matrix,
    increment_speed_offset,
    channel_fading_exponent,
    extra_damping_spikes,
    content_smoothing_coefficients,
    address_smoothing_coefficients,
    newest_lookup_matrix,
    newest_output_switch,
    cluster_scaling_coefficients,
):
    bf16, f32 = jnp.bfloat16, jnp.float32
    anywhere = pl.BlockSpec(memory_space=pltpu.HBM)
    dma = pltpu.SemaphoreType.DMA
    kv, read = pl.pallas_call(
        kernel,
        out_shape=(
            pltpu.VMEM((N * SPAN, LANES), bf16),
            jax.ShapeDtypeStruct((1, HEAD), bf16),
        ),
        in_specs=[anywhere] * 4 + [pl.BlockSpec(memory_space=pltpu.SMEM)] * 2 + [anywhere] * 6,
        out_specs=(pl.BlockSpec(memory_space=pltpu.VMEM),) * 2,
        scratch_shapes=[
            pltpu.VMEM((SPAN, MODEL), bf16),
            pltpu.VMEM((5, MODEL, 256), bf16),
            pltpu.VMEM((HEADS, MODEL), bf16),
            pltpu.VMEM((LANES, LANES), f32),
            pltpu.VMEM((KERNEL, 1, HEAD), f32),
            pltpu.VMEM((KERNEL, GROUPS, STATE), f32),
            pltpu.VMEM((GROUPS, STATE), bf16),
            pltpu.VMEM((1, HEAD), bf16),
            pltpu.VMEM((1, HEAD), f32),
            pltpu.VMEM((SPAN, 256), f32),
            pltpu.VMEM((20, HALF, LANES), bf16),
            pltpu.VMEM((N, HALF, LANES), bf16),
            pltpu.VMEM((N, HALF + NOTE, LANES), bf16),
            pltpu.VMEM((Z, NOTE, LANES), f32),
            pltpu.VMEM((Z, NOTE, LANES), bf16),
            pltpu.VMEM((N + 2, 8, LANES), f32),
            pltpu.VMEM((N + 2, 8, LANES), f32),
            pltpu.VMEM((LANES, LANES), f32),
            pltpu.VMEM((24 * N, LANES), f32),
            pltpu.VMEM((24, HALF), bf16),
            pltpu.VMEM((LANES, HALF), f32),
            pltpu.VMEM((HALF + 16, LANES), f32),
            pltpu.VMEM((HALF + 16, LANES), f32),
            pltpu.VMEM((8, LANES), f32),
            pltpu.VMEM((8, LANES), f32),
            pltpu.VMEM((HALF, LANES), bf16),
            pltpu.VMEM((N, HALF, LANES), bf16),
            pltpu.VMEM((LANES, LANES), f32),
            pltpu.VMEM((LANES, LANES), f32),
            pltpu.VMEM((8, LANES), f32),
            pltpu.VMEM((Y, 8, LANES), f32),
            dma((9,)),
            dma((7,)),
            dma((2 * Z,)),
            dma((Z,)),
            dma((N,)),
            dma((N,)),
            dma((N,)),
            dma((N,)),
            dma((N,)),
            dma((Y,)),
            dma((Y,)),
            dma((N,)),
            pltpu.SemaphoreType.REGULAR((Z,)),
        ],
        compiler_params=pltpu.CompilerParams(
            collective_id=0, has_side_effects=True, vmem_limit_bytes=36 * 1024 * 1024
        ),
        name="mixer",
    )(
        *map(
            in_hbm,
            (
                context_input_tensor[0],
                content_mapping_matrix,
                address_mapping_matrix,
                increment_mapping_matrix.T,
            ),
        ),
        increment_speed_offset,
        channel_fading_exponent,
        *map(
            in_hbm,
            (
                extra_damping_spikes.reshape(LANES, LANES),
                content_smoothing_coefficients,
                address_smoothing_coefficients,
                newest_lookup_matrix[0],
                newest_output_switch[0],
                cluster_scaling_coefficients,
            ),
        ),
    )
    return (kv.reshape(1, N * SPAN, 1, LANES), read[None])


def solution(mesh):
    placed = (
        P(("gr", "tp"), "sp", None),
        P(),
        P(),
        P(),
        P("sp"),
        P("sp"),
        P(("gr", "tp"), "sp", None),
        P(None, "sp", None),
        P(),
        P(("gr", "tp"), None, None),
        P(("gr", "tp"), "sp", None),
        P("sp", None),
    )
    return jax.shard_map(
        on_device,
        mesh=mesh,
        in_specs=placed,
        out_specs=(P(("gr", "tp"), None, "sp", None), P(("gr", "tp"), "sp", None)),
        check_vma=False,
    )
```

```python
import functools

import jax
import jax.numpy as jnp
from jax import lax
from jax.experimental import pallas as pl
from jax.experimental.pallas import tpu as pltpu
from jax.sharding import PartitionSpec as P

HEADS = 16
HEAD = 64
GROUPS = 4
STATE = 64
KERNEL = 5
MODEL = 2048
SPAN = 1024
HALF = SPAN // 2
N = 16
Z = 4
Y = 4
LANES = 128
EPS = 1e-05
MESH = pl.DeviceIdType.MESH
CHUNK = 64
NOTE = 48
CUT = 288
PART = HALF // 2
PIECES = 4


def mirror(place, side):
    return place + side * (3 - 2 * place)


def silu(v):
    half = 0.5 * v
    return half + half * jnp.tanh(half)


def kernel(
    x_hbm,
    wv_hbm,
    wk_hbm,
    wr_hbm,
    offset_ref,
    fading_ref,
    spikes_hbm,
    vtaps_hbm,
    ktaps_hbm,
    query_hbm,
    switch_hbm,
    gain_hbm,
    kv_out,
    read_out,
    xb,
    wb,
    wr,
    spikes,
    vtaps_s,
    ktaps_s,
    query_s,
    switch_s,
    gain_s,
    acc,
    sb,
    rv,
    rk,
    notes,
    nsend,
    edge_v,
    edge_k,
    rates,
    weights,
    chooser,
    spread,
    extv,
    extk,
    tapv,
    tapk,
    vw,
    kc,
    states,
    qmat,
    gsend,
    grecv,
    in_sem,
    small_sem,
    k_send,
    n_send,
    v_send,
    f_send,
    k_recv,
    n_recv,
    v_recv,
    g_send,
    g_recv,
    h_recv,
    ready,
):
    me = lax.axis_index("sp")
    z = me // Y
    y = me % Y
    core = lax.axis_index("tp") % 2
    side = z // 2
    zr = mirror(z, side)

    first = 3 - 2 * (1 - core) * (1 - zr)
    second = (1 - zr) * (3 - 2 * core) + 2 * zr
    third = 2 * (1 - zr)
    steps = [mirror(first, side), mirror(second, side), mirror(third, side), z]

    barrier = pltpu.get_barrier_semaphore()
    column = [((z + i) % Z) * Y + y for i in range(1, Z)]
    row = [z * Y + (y + i) % Y for i in range(1, Y)]
    for peer in column + row:
        pl.semaphore_signal(barrier, inc=1, device_id={"sp": peer}, device_id_type=MESH)

    loads = []
    for i in (0, 2, 1, 3):
        rows = pl.ds(i * PART, PART)
        loads.append(pltpu.make_async_copy(x_hbm.at[rows], xb.at[rows], in_sem.at[i]))
    loads.insert(0, pltpu.make_async_copy(wk_hbm, wb.at[0], in_sem.at[4]))
    for i in range(4):
        cols = pl.ds(pl.multiple_of(steps[i] * 256, 256), 256)
        loads.append(
            pltpu.make_async_copy(wv_hbm.at[:, cols], wb.at[i + 1], in_sem.at[5 + i])
        )
    for c in loads[:5]:
        c.start()
    smalls = [
        pltpu.make_async_copy(a, b, small_sem.at[i])
        for i, (a, b) in enumerate(
            [
                (wr_hbm, wr),
                (spikes_hbm, spikes),
                (vtaps_hbm, vtaps_s),
                (ktaps_hbm, ktaps_s),
                (query_hbm, query_s),
                (switch_hbm, switch_s),
                (gain_hbm, gain_s),
            ]
        )
    ]

    def lo_mask(rows):
        return lax.broadcasted_iota(jnp.int32, (rows, LANES), 1) < HEAD

    def swap(v):
        return pltpu.roll(v, HEAD, 1)

    def remote(src, dst, ssem, rsem, peer):
        return pltpu.make_async_remote_copy(
            src_ref=src,
            dst_ref=dst,
            send_sem=ssem,
            recv_sem=rsem,
            device_id={"sp": peer},
            device_id_type=MESH,
        )

    keys = (pl.ds(0, PART), pl.ds(PART, PART))
    extra = pl.ds(HALF, NOTE)

    def key_copy(zd, part):
        return remote(
            sb.at[zd, keys[part]],
            rk.at[me, keys[part]],
            k_send.at[part * Z + zd],
            (k_recv, h_recv)[part].at[me],
            zd * Y + y,
        )

    def note_copy(zd):
        return remote(
            nsend.at[zd], rk.at[me, extra], n_send.at[zd], n_recv.at[me], zd * Y + y
        )

    def value_copy(slot, dest):
        return remote(sb.at[slot], rv.at[me], v_send.at[dest], v_recv.at[me], dest)

    def step_copy(zs, way):
        s = zs * Y + y
        return remote(
            rk.at[s],
            rk.at[s],
            f_send.at[zs * Y + (1 - way) // 2],
            k_recv.at[s],
            z * Y + (y + way) % Y,
        )

    def half_copy(zs, way):
        s = zs * Y + (y - way) % Y
        part = pl.ds(0, CUT) if way == 1 else pl.ds(CUT, HALF + NOTE - CUT)
        return remote(
            rk.at[s, part],
            rk.at[s, part],
            f_send.at[zs * Y + 2 + (1 - way) // 2],
            k_recv.at[s] if way == 1 else n_recv.at[s],
            z * Y + (y + way) % Y,
        )

    def multiply(i):
        acc[...] = jnp.dot(xb[...], wb[i], preferred_element_type=jnp.float32)
        pack(i, 0, HALF)

    def pack(i, start, stop):
        low = lo_mask(CHUNK)
        for r0 in range(start, stop, CHUNK):
            for pair in range(2):
                cols = slice(pair * LANES, (pair + 1) * LANES)
                top = acc[r0 : r0 + CHUNK, cols]
                bot = acc[r0 + HALF : r0 + HALF + CHUNK, cols]
                even = jnp.where(low, top, swap(bot))
                odd = jnp.where(low, swap(top), bot)
                sb[4 * i + 2 * pair, r0 : r0 + CHUNK] = even.astype(jnp.bfloat16)
                sb[4 * i + 2 * pair + 1, r0 : r0 + CHUNK] = odd.astype(jnp.bfloat16)

    low8 = lo_mask(8)

    def edge_rows(head, tail):
        out = []
        for pair in range(2):
            cols = slice(pair * LANES, (pair + 1) * LANES)
            top = head[:, cols]
            bot = pltpu.roll(tail[:, cols], 2, 0)
            out.append(jnp.where(low8, bot, swap(top))[0:2])
            out.append(jnp.where(low8, swap(bot), top)[0:2])
        return out

    notes[...] = jnp.zeros_like(notes)

    for part in range(2):
        for c in loads[2 * part + (part > 0) : 2 * part + 3]:
            c.wait()
        if part == 1:
            for c in loads[5:] + smalls:
                c.start()
        for r0 in (PART * part, HALF + PART * part):
            acc[r0 : r0 + PART] = jnp.dot(
                xb[r0 : r0 + PART], wb[0], preferred_element_type=jnp.float32
            )
        pack(0, PART * part, PART * part + PART)
        if part == 0:
            pl.semaphore_wait(barrier, Z + Y - 2)
            for peer in column:
                pl.semaphore_signal(
                    ready.at[z], inc=1, device_id={"sp": peer}, device_id_type=MESH
                )
        for k in range(3):
            key_copy(steps[k], part).start()
    rk[me, 0:HALF] = sb[z]

    for g, e in enumerate(edge_rows(acc[0:8], acc[SPAN - 8 : SPAN])):
        notes[g, 40:42] = e
    for c in loads[5:] + smalls:
        c.wait()
    xe = jnp.concatenate([xb[0:16], xb[SPAN - 16 : SPAN]], axis=0)
    for i in range(1, 5):
        e32 = jnp.dot(xe, wb[i], preferred_element_type=jnp.float32)
        for j, e in enumerate(edge_rows(e32[0:8], e32[24:32])):
            notes[steps[i - 1], 32 + 2 * j : 34 + 2 * j] = e
    raw = lax.dot_general(
        wr[...], xb[...], (((1,), (1,)), ((), ())), preferred_element_type=jnp.float32
    )
    for b in range(8):
        block = raw[:, b * LANES : (b + 1) * LANES]
        for h in range(HEADS):
            row = 8 * (h % Y) + b
            notes[h // Y, row : row + 1] = block[h : h + 1]
    nsend[...] = notes[...].astype(jnp.bfloat16)
    for k in range(3):
        note_copy(steps[k]).start()
    rk[me, HALF:] = nsend[z]
    for way in (1, -1):
        step_copy(z, way).start()

    def tile(i, carry):
        multiply(i)
        zd = steps[0] * (i == 1) + steps[1] * (i == 2) + steps[2] * (i == 3) + z * (i == 4)

        @pl.when(i < 4)
        def _():
            pl.semaphore_wait(ready.at[zd], 1)
            for j in (2, 1, 3, 0):
                yd = (y + j) % Y
                value_copy(4 * i + yd, zd * Y + yd).start()

        return carry

    lax.fori_loop(1, 5, tile, 0)
    rv[me] = sb[16 + y]

    def pass_on(zs):
        for way in (1, -1):
            s = zs * Y + (y - way) % Y
            remote(rk.at[0], rk.at[s], f_send.at[0], k_recv.at[s], s).wait_recv()
            half_copy(zs, way).start()

    places = [z, mirror(1 - zr, side), mirror(2 + 0 * zr, side), mirror(3 + 0 * zr, side)]
    for i in range(1, 4):
        s = places[i] * Y + y
        for part, sem in ((keys[0], k_recv), (keys[1], h_recv)):
            remote(sb.at[0, part], rk.at[s, part], k_send.at[0], sem.at[s], s).wait_recv()
        remote(nsend.at[0], rk.at[s, extra], n_send.at[0], n_recv.at[s], s).wait_recv()
        for way in (1, -1):
            step_copy(places[i], way).start()
        pass_on(places[i - 1])
    pass_on(places[3])
    for j in (2, 1, 3):
        yd = (y + j) % Y
        value_copy(16 + yd, z * Y + yd).start()
    for zz in range(Z):
        s = zz * Y + (y + 2) % Y
        part = pl.ds(0, CUT)
        remote(rk.at[0, part], rk.at[s, part], f_send.at[0], k_recv.at[s], s).wait_recv()
        part = pl.ds(CUT, HALF + NOTE - CUT)
        remote(rk.at[0, part], rk.at[s, part], f_send.at[0], n_recv.at[s], s).wait_recv()

    edge_v[0] = jnp.zeros((8, LANES), jnp.float32)
    edge_k[0] = jnp.zeros((8, LANES), jnp.float32)
    edge_v[N + 1] = jnp.zeros((8, LANES), jnp.float32)
    edge_k[N + 1] = jnp.zeros((8, LANES), jnp.float32)
    row8 = lax.broadcasted_iota(jnp.int32, (8, LANES), 0)

    def unpack(s, carry):
        got = rk[s, HALF:].astype(jnp.float32)
        mine = got[0:8] * (y == 0) + got[8:16] * (y == 1)
        mine = mine + got[16:24] * (y == 2) + got[24:32] * (y == 3)
        rates[pl.ds(pl.multiple_of(8 * s, 8), 8)] = mine
        ends = got[32:40]
        e0 = jnp.sum(jnp.where(row8 == 2 * y, ends, 0.0), axis=0, keepdims=True)
        e1 = jnp.sum(jnp.where(row8 == 2 * y + 1, ends, 0.0), axis=0, keepdims=True)
        even = row8 % 2 == 0
        edge_v[s + 1] = jnp.where(even, e0, e1)
        edge_k[s + 1] = jnp.where(even, got[40:41], got[41:42])
        return carry

    lax.fori_loop(0, N, unpack, 0, unroll=4)
    speed = rates[...] + offset_ref[0]
    speed = jnp.maximum(speed, 0.0) + jnp.log1p(jnp.exp(-jnp.abs(speed)))
    log_step = -jnp.exp(jnp.full((1, LANES), fading_ref[0], jnp.float32)) * speed + spikes[...]
    ri = lax.broadcasted_iota(jnp.int32, (LANES, LANES), 0)
    ci = lax.broadcasted_iota(jnp.int32, (LANES, LANES), 1)
    later_lane = (ri > ci).astype(jnp.float32)
    later_row = (ci > ri).astype(jnp.float32)
    inner = jnp.dot(
        log_step, later_lane, precision=lax.Precision.HIGHEST, preferred_element_type=jnp.float32
    )
    outer = jnp.dot(
        later_row, log_step, precision=lax.Precision.HIGHEST, preferred_element_type=jnp.float32
    )
    suffix = inner + jnp.sum(outer, axis=1, keepdims=True)
    weight = speed * jnp.exp(suffix)
    for part in range(3):
        piece = weight.astype(jnp.bfloat16).astype(jnp.float32)
        weight = weight - piece
        for s in range(N):
            weights[24 * s + 8 * part : 24 * s + 8 * part + 8] = piece[8 * s : 8 * s + 8]
    shape = (24, HALF)
    wanted = lax.broadcasted_iota(jnp.int32, shape, 1)
    wanted = wanted // LANES + Y * (wanted % LANES >= HEAD)
    pick = lax.broadcasted_iota(jnp.int32, shape, 0) % 8 == wanted
    chooser[...] = pick.astype(jnp.float32).astype(jnp.bfloat16)

    for k in range(KERNEL):
        row = vtaps_s[k]
        tapv[k : k + 1, :] = jnp.concatenate([row, row], axis=1)
        row = ktaps_s[k, pl.ds(z, 1), :]
        tapk[k : k + 1, :] = jnp.concatenate([row, row], axis=1)
    qrow = query_s[...].astype(jnp.float32)
    pick = lax.broadcasted_iota(jnp.int32, (GROUPS, STATE), 0) == z
    qrow = jnp.sum(jnp.where(pick, qrow, 0.0), axis=0, keepdims=True)
    qrow = jnp.concatenate([qrow, qrow], axis=1)
    qcol = jnp.transpose(jnp.broadcast_to(qrow, (LANES, LANES)))
    qmat[...] = jnp.where((ri < STATE) == (ci < HEAD), qcol, 0.0)
    states[...] = jnp.zeros_like(states)

    def span_of(t):
        zi = t // Y
        ji = t % Y
        place = 3 * (zi == 0) + (1 - zr) * 2 * (zi == 1) + (zi == 2) + zr * 2 * (zi == 3)
        zz = mirror(place, side)
        j = 2 * (ji == 0) + 3 * (ji == 1) + (ji == 2)
        return zz * Y + (y + j) % Y

    low_c = lo_mask(CHUNK)

    def extend(block, edge, s, ext):
        block = block.astype(jnp.float32)
        ext[8 : 8 + HALF] = block
        ext[0:8] = jnp.where(low8, edge[s], swap(block[HALF - 8 : HALF]))
        ext[8 + HALF : 16 + HALF] = jnp.where(low8, swap(block[0:8]), edge[s + 2])

    def convolved(ext, tap, r0):
        total = tap[0:1] * ext[r0 + 6 : r0 + 6 + CHUNK]
        for k in range(1, KERNEL):
            total = total + tap[k : k + 1] * ext[r0 + 6 + k : r0 + 6 + k + CHUNK]
        return silu(total)

    def convolve_keys(s, carry):
        extend(rk[s, 0:HALF], edge_k, s, extk)
        for r0 in range(0, HALF, CHUNK):
            kc[s, r0 : r0 + CHUNK] = convolved(extk, tapk, r0).astype(jnp.bfloat16)
        return carry

    lax.fori_loop(0, N, convolve_keys, 0)

    def write_rows(s, r0, v):
        base = pl.multiple_of(s * SPAN, SPAN) + r0
        k = kc[s, r0 : r0 + CHUNK].astype(jnp.float32)
        kv_out[pl.ds(base, CHUNK)] = jnp.where(low_c, v, swap(k)).astype(jnp.bfloat16)
        kv_out[pl.ds(base + HALF, CHUNK)] = jnp.where(low_c, swap(v), k).astype(jnp.bfloat16)

    def process(t, write):
        s = span_of(t)

        @pl.when(s != me)
        def _():
            remote(sb.at[0], rv.at[s], v_send.at[0], v_recv.at[s], s).wait_recv()

        extend(rv[s], edge_v, s, extv)
        parts = weights[pl.ds(pl.multiple_of(24 * s, 8), 24)].astype(jnp.bfloat16)
        spread[...] = lax.dot_general(
            parts, chooser[...], (((0,), (0,)), ((), ())), preferred_element_type=jnp.float32
        )
        for r0 in range(0, HALF, CHUNK):
            v = convolved(extv, tapv, r0)
            b = r0 // LANES
            p0 = r0 % LANES
            w = spread[p0 : p0 + CHUNK, b * LANES : (b + 1) * LANES]
            vw[r0 : r0 + CHUNK] = (v * w).astype(jnp.bfloat16)
            if write:
                write_rows(s, r0, v)
            else:
                rv[s, r0 : r0 + CHUNK] = v.astype(jnp.bfloat16)
        states[...] += lax.dot_general(
            kc[s], vw[...], (((0,), (0,)), ((), ())), preferred_element_type=jnp.float32
        )

    def process_step(t, carry):
        process(t, True)
        return carry

    lax.fori_loop(0, N - 1, process_step, 0)
    process(N - 1, False)

    read = jnp.sum(states[...] * qmat[...], axis=0, keepdims=True)
    read = read + swap(read)
    gate = switch_s[...].astype(jnp.float32)
    gate = jnp.concatenate([gate, gate], axis=1)
    gated = read * silu(gate)
    square = 0.5 * jnp.sum(gated * gated, axis=1, keepdims=True)
    gsend[...] = jnp.broadcast_to(square, (8, LANES))

    def square_copy(j):
        return remote(
            gsend, grecv.at[y], g_send.at[j], g_recv.at[y], z * Y + (y + j) % Y
        )

    for j in (2, 1, 3):
        square_copy(j).start()
    grecv[y] = gsend[...]
    last = span_of(N - 1)
    for r0 in range(0, HALF, CHUNK):
        write_rows(last, r0, rv[last, r0 : r0 + CHUNK].astype(jnp.float32))
    for j in (1, 2, 3):
        yy = (y + j) % Y
        remote(gsend, grecv.at[yy], g_send.at[0], g_recv.at[yy], me).wait_recv()
    total = grecv[0] + grecv[1] + grecv[2] + grecv[3]
    gain = gain_s[...]
    gain = jnp.concatenate([gain, gain], axis=1)
    scaled = gated * lax.rsqrt(total[0:1] / (HEAD * HEADS // GROUPS) + EPS) * gain
    read_out[...] = scaled[:, :HEAD].astype(jnp.bfloat16)

    for j in (1, 2, 3):
        square_copy(j).wait_send()
        value_copy(16, z * Y + (y + j) % Y).wait_send()
    for k in range(3):
        for part in range(2):
            key_copy(steps[k], part).wait_send()
        note_copy(steps[k]).wait_send()
        for j in range(Y):
            value_copy(4, steps[k] * Y + j).wait_send()
    for zs in range(Z):
        for way in (1, -1):
            step_copy(zs, way).wait_send()
            half_copy(zs, way).wait_send()


def hand_out(kv_in, read_in, kv_out, read_out, sem):
    size = N * SPAN // PIECES
    copies = [pltpu.make_async_copy(read_in, read_out, sem.at[PIECES])]
    for i in range(PIECES):
        rows = pl.ds(i * size, size)
        copies.append(pltpu.make_async_copy(kv_in.at[rows], kv_out.at[rows], sem.at[i]))
    for c in copies:
        c.start()
    for c in copies:
        c.wait()


def in_hbm(a):
    return pltpu.with_memory_space_constraint(a, pltpu.HBM)


def on_device(
    context_input_tensor,
    content_mapping_matrix,
    address_mapping_matrix,
    increment_mapping_matrix,
    increment_speed_offset,
    channel_fading_exponent,
    extra_damping_spikes,
    content_smoothing_coefficients,
    address_smoothing_coefficients,
    newest_lookup_matrix,
    newest_output_switch,
    cluster_scaling_coefficients,
):
    bf16, f32 = jnp.bfloat16, jnp.float32
    anywhere = pl.BlockSpec(memory_space=pltpu.HBM)
    dma = pltpu.SemaphoreType.DMA
    kv, read = pl.pallas_call(
        kernel,
        out_shape=(
            pltpu.VMEM((N * SPAN, LANES), bf16),
            jax.ShapeDtypeStruct((1, HEAD), bf16),
        ),
        in_specs=[anywhere] * 4 + [pl.BlockSpec(memory_space=pltpu.SMEM)] * 2 + [anywhere] * 6,
        out_specs=(pl.BlockSpec(memory_space=pltpu.VMEM),) * 2,
        scratch_shapes=[
            pltpu.VMEM((SPAN, MODEL), bf16),
            pltpu.VMEM((5, MODEL, 256), bf16),
            pltpu.VMEM((HEADS, MODEL), bf16),
            pltpu.VMEM((LANES, LANES), f32),
            pltpu.VMEM((KERNEL, 1, HEAD), f32),
            pltpu.VMEM((KERNEL, GROUPS, STATE), f32),
            pltpu.VMEM((GROUPS, STATE), bf16),
            pltpu.VMEM((1, HEAD), bf16),
            pltpu.VMEM((1, HEAD), f32),
            pltpu.VMEM((SPAN, 256), f32),
            pltpu.VMEM((20, HALF, LANES), bf16),
            pltpu.VMEM((N, HALF, LANES), bf16),
            pltpu.VMEM((N, HALF + NOTE, LANES), bf16),
            pltpu.VMEM((Z, NOTE, LANES), f32),
            pltpu.VMEM((Z, NOTE, LANES), bf16),
            pltpu.VMEM((N + 2, 8, LANES), f32),
            pltpu.VMEM((N + 2, 8, LANES), f32),
            pltpu.VMEM((LANES, LANES), f32),
            pltpu.VMEM((24 * N, LANES), f32),
            pltpu.VMEM((24, HALF), bf16),
            pltpu.VMEM((LANES, HALF), f32),
            pltpu.VMEM((HALF + 16, LANES), f32),
            pltpu.VMEM((HALF + 16, LANES), f32),
            pltpu.VMEM((8, LANES), f32),
            pltpu.VMEM((8, LANES), f32),
            pltpu.VMEM((HALF, LANES), bf16),
            pltpu.VMEM((N, HALF, LANES), bf16),
            pltpu.VMEM((LANES, LANES), f32),
            pltpu.VMEM((LANES, LANES), f32),
            pltpu.VMEM((8, LANES), f32),
            pltpu.VMEM((Y, 8, LANES), f32),
            dma((9,)),
            dma((7,)),
            dma((2 * Z,)),
            dma((Z,)),
            dma((N,)),
            dma((N,)),
            dma((N,)),
            dma((N,)),
            dma((N,)),
            dma((Y,)),
            dma((Y,)),
            dma((N,)),
            pltpu.SemaphoreType.REGULAR((Z,)),
        ],
        compiler_params=pltpu.CompilerParams(
            collective_id=0, has_side_effects=True, vmem_limit_bytes=36 * 1024 * 1024
        ),
        name="mixer",
    )(
        *map(
            in_hbm,
            (
                context_input_tensor[0],
                content_mapping_matrix,
                address_mapping_matrix,
                increment_mapping_matrix.T,
            ),
        ),
        increment_speed_offset,
        channel_fading_exponent,
        *map(
            in_hbm,
            (
                extra_damping_spikes.reshape(LANES, LANES),
                content_smoothing_coefficients,
                address_smoothing_coefficients,
                newest_lookup_matrix[0],
                newest_output_switch[0],
                cluster_scaling_coefficients,
            ),
        ),
    )
    on_chip = pl.BlockSpec(memory_space=pltpu.VMEM)
    kv, read = pl.pallas_call(
        hand_out,
        out_shape=(
            jax.ShapeDtypeStruct((N * SPAN, LANES), bf16),
            jax.ShapeDtypeStruct((1, HEAD), bf16),
        ),
        in_specs=[on_chip, on_chip],
        out_specs=(anywhere, anywhere),
        scratch_shapes=[dma((PIECES + 1,))],
        compiler_params=pltpu.CompilerParams(vmem_limit_bytes=8 * 1024 * 1024),
        name="hand_out",
    )(*(pltpu.with_memory_space_constraint(a, pltpu.VMEM) for a in (kv, read)))
    return (kv.reshape(1, N * SPAN, 1, LANES), read[None])


def solution(mesh):
    placed = (
        P(("gr", "tp"), "sp", None),
        P(),
        P(),
        P(),
        P("sp"),
        P("sp"),
        P(("gr", "tp"), "sp", None),
        P(None, "sp", None),
        P(),
        P(("gr", "tp"), None, None),
        P(("gr", "tp"), "sp", None),
        P("sp", None),
    )
    return jax.shard_map(
        on_device,
        mesh=mesh,
        in_specs=placed,
        out_specs=(P(("gr", "tp"), None, "sp", None), P(("gr", "tp"), "sp", None)),
        check_vma=False,
    )
```
